256 devices in a mesh: grp: 2 (over y), sp: 32 (over z, core), tp: 4 (over x).
Axes of the slice: x: 4, y: 2, z: 16, core: 2. Of those that a mesh axis runs over, the one named last changes fastest.
The devices are a block of a 4x16x16 slice.
Arguments:
- resid_in: bfloat16 [16384, 2048], P(('grp', 'sp', 'tp')), parts along dimension 0, may hold values from -6 to 6
- query_narrow: bfloat16 [16384, 8, 128], P(('grp', 'sp'), 'tp'), parts along dimension 0, may hold values from -512 to 512
- key_narrow: bfloat16 [16384, 4, 128], P(('grp', 'sp'), 'tp'), parts along dimension 0, may hold values from -512 to 512
- value_narrow: bfloat16 [16384, 4, 128], P(('grp', 'sp'), 'tp'), parts along dimension 0, may hold values from -6 to 6
- query_wide: bfloat16 [16384, 8, 256], P(('grp', 'sp'), 'tp'), parts along dimension 0, may hold values from -512 to 512
- key_wide: bfloat16 [16384, 4, 256], P(('grp', 'sp'), 'tp'), parts along dimension 0, may hold values from -512 to 512
- value_wide: bfloat16 [16384, 4, 128], P(('grp', 'sp'), 'tp'), parts along dimension 0, may hold values from -6 to 6
- lambda_narrow: float32 [8], P('tp'), may hold values from 0.3 to 0.8
- lambda_wide: float32 [8], P('tp'), may hold values from 0.3 to 0.8
- head_gain: float32 [128], replicated, may hold values from 0.1 to 1.9
- out_narrow: bfloat16 [1024, 2048], P('tp'), may hold values from -0.125 to 0.125
- out_wide: bfloat16 [1024, 2048], P('tp'), may hold values from -0.125 to 0.125
- norm_gain: bfloat16 [2048], replicated, may hold values from 0.099609375 to 1.8984375
- up_weight: bfloat16 [2048, 8192], P('sp', 'tp'), may hold values from -0.125 to 0.125
- down_weight: bfloat16 [8192, 2048], P('tp', 'sp'), may hold values from -0.0625 to 0.0625
Outputs:
- mixed_out: bfloat16 [16384, 2048], P(('grp', 'sp', 'tp')), parts along dimension 0
The draws below stay inside these ranges and needn't reach their ends.
There are 2 independent parts, one for each index of `grp`. The reference program is written for one: setup_inputs(seed, part) draws one part's arguments, and reference() takes and returns one part's arrays. A program takes and returns all parts, laid end to end along the dimension named above; an argument that names none is the same for every part. Nothing has to cross between parts.
All inputs are finite; a program needn't handle non-finite values.
Results may differ from the reference program's by a relative error of at most 0.018.
Values may be sent and summed in bfloat16 or wider, within the bound.
A program may use at most 128 MiB of HBM per device.

```python
import math
import jax
import jax.numpy as jnp
from jax import lax

D = 2048
FF = 8192
HN = 8
DN = 64
KN = 4
HW = 8
DW = 128
KW = 4
DV = 128
SEQ = 8192
N_TP = 4


SPREAD = 1.32


def paired_draw(base_key, head_count, key_head_stack, half_width):
    full_width = 2 * half_width
    query_draw, keys_draw = jax.random.split(base_key, 2)
    key_rows = jnp.clip(jax.random.normal(keys_draw, (SEQ, key_head_stack, full_width), jnp.float32) * SPREAD, -4.0 * SPREAD, 4.0 * SPREAD)
    query_rows_all = jnp.clip(jax.random.normal(query_draw, (SEQ, head_count, full_width), jnp.float32) * SPREAD, -4.0 * SPREAD, 4.0 * SPREAD)
    return (query_rows_all, key_rows)


def draw_query_narrow(key, part):
    return paired_draw(jax.random.fold_in(key, 101), HN, KN, DN)[0].astype(jnp.bfloat16)


def draw_key_narrow(key, part):
    return paired_draw(jax.random.fold_in(key, 101), HN, KN, DN)[1].astype(jnp.bfloat16)


def draw_query_wide(key, part):
    return paired_draw(jax.random.fold_in(key, 202), HW, KW, DW)[0].astype(jnp.bfloat16)


def draw_key_wide(key, part):
    return paired_draw(jax.random.fold_in(key, 202), HW, KW, DW)[1].astype(jnp.bfloat16)


def steps_of(rng, shape, cuts, smallest, high):
    level = 1.0
    for dim, shards_of in cuts:
        steps = jax.random.uniform(jax.random.fold_in(jax.random.fold_in(rng, 6), dim), (shards_of,), jnp.float32, smallest / len(cuts), high / len(cuts))
        level = level * jnp.repeat(jnp.exp(steps), shape[dim] // shards_of).reshape((-1,) + (1,) * (len(shape) - 1 - dim))
    return level


def scatter_about(key, dims, spread, limit, cuts=(), held_as=jnp.bfloat16):
    result = jax.random.normal(key, dims, jnp.float32) * spread
    if len(cuts) > 0:
        result = steps_of(key, dims, cuts, -0.22, 0.18) * result
    return jnp.clip(result, min=-limit, max=limit).astype(held_as)


def setup_inputs(seed: int = 0, part: int = 0) -> dict:
    streams_of = jax.random.split(jax.random.key(seed), 16)
    part_splits = jax.random.split(jax.random.fold_in(streams_of[15], part), 16)
    return {
        "resid_in": scatter_about(part_splits[0], (SEQ, D), 1.0, 6.0, ((0, 128),)),
        "query_narrow": draw_query_narrow(jax.random.fold_in(jax.random.fold_in(streams_of[15], part), 71), part),
        "key_narrow": draw_key_narrow(jax.random.fold_in(jax.random.fold_in(streams_of[15], part), 71), part),
        "value_narrow": scatter_about(part_splits[3], (SEQ, KN, DV), 1.0, 6.0, ((0, 32), (1, 4))),
        "query_wide": draw_query_wide(jax.random.fold_in(jax.random.fold_in(streams_of[15], part), 71), part),
        "key_wide": draw_key_wide(jax.random.fold_in(jax.random.fold_in(streams_of[15], part), 71), part),
        "value_wide": scatter_about(part_splits[6], (SEQ, KW, DV), 1.0, 6.0, ((0, 32), (1, 4))),
        "lambda_narrow": jnp.clip(0.3 + 0.5 * jax.random.uniform(streams_of[7], (HN,), jnp.float32) ** steps_of(streams_of[7], (HN,), ((0, 4),), -0.2, 0.2), 0.3, 0.8),
        "lambda_wide": jnp.clip(0.3 + 0.5 * jax.random.uniform(streams_of[8], (HW,), jnp.float32) ** steps_of(streams_of[8], (HW,), ((0, 4),), -0.2, 0.2), 0.3, 0.8),
        "head_gain": jnp.clip(1.0 + 0.18 * jax.random.normal(streams_of[9], (DV,), jnp.float32), 0.1, 1.9),
        "out_narrow": scatter_about(streams_of[10], (HN * DV, D), ((HN + HW) * DV) ** -0.5, 0.125, ((0, 4),)),
        "out_wide": scatter_about(streams_of[11], (HW * DV, D), ((HN + HW) * DV) ** -0.5, 0.125, ((0, 4),)),
        "norm_gain": jnp.clip(1.0 + 0.18 * jax.random.normal(streams_of[12], (D,), jnp.float32), 0.099609375, 1.8984375).astype(jnp.bfloat16),
        "up_weight": scatter_about(streams_of[13], (D, FF), D ** -0.5, 0.125, ((0, 32), (1, 4))),
        "down_weight": scatter_about(streams_of[14], (FF, D), FF ** -0.5, 0.0625, ((0, 4), (1, 32))),
    }


NORM_EPS = 1e-06
OUT_SCALE = 0.8

def attend_ref(query, key_rows, values, lambdas, gain_vec):
    seq_len, head_count, full_width = query.shape
    key_head_stack = key_rows.shape[1]
    half_width = full_width // 2
    group_size = head_count // key_head_stack
    value_width = values.shape[2]
    block_rows = math.gcd(seq_len, 128)
    rotation_count = seq_len // block_rows
    key_float32 = key_rows.astype(jnp.float32).reshape(seq_len, key_head_stack, 2, half_width)
    value_float32 = values.astype(jnp.float32)
    query_blocks = query.reshape(rotation_count, block_rows, key_head_stack, group_size, 2, half_width)
    lambda_grid = lambdas.reshape(key_head_stack, group_size)[:, :, None, None]

    def per_block(query_blk):
        scores = jnp.einsum('tkgcd,skcd->kgcts', query_blk.astype(jnp.float32), key_float32) * half_width ** (-0.5)
        row_top = lax.optimization_barrier(jnp.max(scores, axis=-1, keepdims=True))
        powers = jnp.exp(scores - row_top)
        row_total = lax.optimization_barrier(jnp.sum(powers, axis=-1))
        rounded_result = lax.optimization_barrier(powers.astype(jnp.bfloat16)).astype(jnp.float32)
        weighted_values = jnp.einsum('iodph,hie->iodpe', rounded_result, value_float32)
        first_map = weighted_values[:, :, 0] / row_total[:, :, 0, :, None]
        second_map = weighted_values[:, :, 1] / row_total[:, :, 1, :, None]
        mixed = first_map - lambda_grid * second_map
        normed = mixed * lax.rsqrt(lax.optimization_barrier(jnp.mean(mixed * mixed, axis=-1, keepdims=True)) + NORM_EPS) * gain_vec * OUT_SCALE
        normed = normed.astype(jnp.bfloat16).transpose(2, 0, 1, 3)
        return normed.reshape(block_rows, head_count, value_width)
    outcome = lax.map(per_block, query_blocks)
    return outcome.reshape(seq_len, head_count * value_width)

def rounded_add(running, partial_value):
    return running + lax.optimization_barrier(partial_value.astype(jnp.bfloat16)).astype(jnp.float32)

def reference(resid_in, query_narrow, key_narrow, value_narrow, query_wide, key_wide, value_wide, lambda_narrow, lambda_wide, head_gain, out_narrow, out_wide, norm_gain, up_weight, down_weight):
    att_narrow = attend_ref(query_narrow, key_narrow, value_narrow, lambda_narrow, head_gain)
    att_wide = attend_ref(query_wide, key_wide, value_wide, lambda_wide, head_gain)
    narrow_cols = att_narrow.shape[1] // N_TP
    wide_cols = att_wide.shape[1] // N_TP
    projected = jnp.zeros(resid_in.shape, jnp.float32)
    for part_index in range(N_TP):
        low_n = part_index * narrow_cols
        low_w = part_index * wide_cols
        partial_value = jnp.dot(att_narrow[:, low_n:low_n + narrow_cols], out_narrow[low_n:low_n + narrow_cols], preferred_element_type=jnp.float32)
        partial_value = partial_value + jnp.dot(att_wide[:, low_w:low_w + wide_cols], out_wide[low_w:low_w + wide_cols], preferred_element_type=jnp.float32)
        projected = rounded_add(projected, partial_value)
    middle = (resid_in.astype(jnp.float32) + projected).astype(jnp.bfloat16)
    middle_f32 = middle.astype(jnp.float32)
    normed = middle_f32 * lax.rsqrt(lax.optimization_barrier(jnp.mean(middle_f32 * middle_f32, axis=-1, keepdims=True)) + NORM_EPS)
    normed = (normed * norm_gain.astype(jnp.float32)).astype(jnp.bfloat16)
    hidden_cols = up_weight.shape[1] // N_TP
    mixer = jnp.zeros(resid_in.shape, jnp.float32)
    for part_index in range(N_TP):
        low_h = part_index * hidden_cols
        lifted = jnp.dot(normed, up_weight[:, low_h:low_h + hidden_cols], preferred_element_type=jnp.float32)
        activated = jnp.square(jax.nn.relu(lifted)).astype(jnp.bfloat16)
        partial_value = jnp.dot(activated, down_weight[low_h:low_h + hidden_cols], preferred_element_type=jnp.float32)
        mixer = rounded_add(mixer, partial_value)
    return (middle_f32 + mixer).astype(jnp.bfloat16)
```

```python
import functools
import math

import jax
import jax.numpy as jnp
from jax import lax
from jax.experimental import pallas as pl
from jax.experimental.pallas import tpu as pltpu
from jax.sharding import PartitionSpec as P

NORM_EPS = 1e-06
OUT_SCALE = 0.8
LOG2E = math.log2(math.e)
MESH = pl.DeviceIdType.MESH
BF16 = jnp.bfloat16
F32 = jnp.float32

KV_N, KV_W, UP, DN_A, DN_B = range(5)
LAST_WAY = (1, 0, 1, 0, 1)
C_KV_N, C_KV_W, C_UP, C_DN = range(4)
CORE_LAST = (1, 0, 1, 1)
Y_UP, Y_DN = range(2)
KEY_PART = (0, 0, 2, 3)
VALUE_PART = (1, 1, 4, 4)
Q_TILE = 128
COLS = 512


def layer_kernel(
    nz, ntp, widths,
    q_ref, kn_ref, vn_ref, kw_ref, vw_ref, up_ref, dn_ref, on_ref, ow_ref, res_ref,
    lam_n_ref, lam_w_ref, head_gain_ref, norm_gain_ref,
    out_ref,
    kv, up, dn, outs, resid, acc, top, att, mid, nrm, act, part, mix, sumsq,
    zs, zr, cs, cr, ys, yr, xs, xr, os_, or_, rs, rr, as_, ar, ms, mr, ls,
):
    g, s, j = lax.axis_index("grp"), lax.axis_index("sp"), lax.axis_index("tp")
    z, c = s // 2, s % 2
    par = g % 2
    half = nz // 2
    rows = kv.shape[2]
    wrows = up.shape[1]
    hrows = wrows // 2
    qrows = wrows // 4
    own_rows = resid.shape[1]

    def sp_of(chip):
        return {"sp": 2 * lax.rem(chip + nz, nz) + c}

    z_to = (sp_of(z + 1), sp_of(z - 1))
    core_to = {"sp": 2 * z + 1 - c}
    y_to = {"grp": g + 1 - 2 * par}

    def tp_at(delta):
        return lax.rem(j + delta + ntp, ntp)

    def chip_at(d, t):
        return lax.rem(z - t + nz, nz) if d == 0 else lax.rem(z + t, nz)

    def piece(kind, block):
        if kind == KV_N:
            return kv.at[block, pl.ds(0, 2)]
        if kind == KV_W:
            return kv.at[block, pl.ds(2, 3)]
        if kind == UP:
            return up.at[block, pl.ds(pl.multiple_of(hrows * par, hrows), hrows)]
        if kind == DN_A:
            return dn.at[block, pl.ds(qrows, hrows)]
        return dn.at[block, pl.ds(pl.multiple_of(3 * qrows * par, qrows), qrows)]

    def remote(src, dst, send, recv, to):
        return pltpu.make_async_remote_copy(src, dst, send, recv, device_id=to, device_id_type=MESH)

    def z_send(kind, d, t):
        ref = piece(kind, 2 * chip_at(d, t) + c)
        return remote(ref, ref, zs.at[kind, d, t], zr.at[kind, d, t + 1], z_to[d])

    def z_recv(kind, d, t):
        ref = piece(kind, 2 * chip_at(d, t) + c)
        return remote(ref, ref, zs.at[kind, d, 0], zr.at[kind, d, t], z_to[d])

    def core_piece(kind, block):
        if kind == C_KV_N:
            return kv.at[block, pl.ds(0, 2)]
        if kind == C_KV_W:
            return kv.at[block, pl.ds(2, 3)]
        return (up if kind == C_UP else dn).at[block]

    def core_send(kind, d, t):
        ref = core_piece(kind, 2 * chip_at(d, t) + c)
        return remote(ref, ref, cs.at[kind, d, t], cr.at[kind, d, t], core_to)

    def core_recv(kind, d, t, chip):
        ref = core_piece(kind, 2 * chip + 1 - c)
        return remote(ref, ref, cs.at[kind, 0, 0], cr.at[kind, d, t], core_to)

    def y_piece(kind, block, side):
        if kind == Y_UP:
            return up.at[block, pl.ds(pl.multiple_of(hrows * side, hrows), hrows)]
        return dn.at[block, pl.ds(pl.multiple_of(3 * qrows * side, qrows), qrows)]

    def y_send(kind, d, t):
        ref = y_piece(kind, 2 * chip_at(d, t) + c, par)
        return remote(ref, ref, ys.at[kind, d, t], yr.at[kind, d, t], y_to)

    def y_recv(kind, d, t):
        ref = y_piece(kind, 2 * chip_at(d, t) + c, 1 - par)
        return remote(ref, ref, ys.at[kind, d, t], yr.at[kind, d, t], y_to)

    def x_send(d):
        ref = outs.at[j, c]
        return remote(ref, ref, xs.at[d], xr.at[d], {"tp": tp_at(1 - 2 * d)})

    def x_recv(d):
        ref = outs.at[tp_at(2 * d - 1), c]
        return remote(ref, ref, xs.at[d], xr.at[d], {"tp": tp_at(1 - 2 * d)})

    def x_half(owner, d):
        n = outs.shape[2] // 2
        return outs.at[owner, c, pl.ds(n * d, n)]

    def x_relay(d):
        ref = x_half(tp_at(2 * d - 1), d)
        return remote(ref, ref, xs.at[2 + d], xr.at[2 + d], {"tp": tp_at(1 - 2 * d)})

    def x_relayed(d):
        ref = x_half(tp_at(2), d)
        return remote(ref, ref, xs.at[2 + d], xr.at[2 + d], {"tp": tp_at(1 - 2 * d)})

    def o_core(delta, mine):
        ref = outs.at[tp_at(delta), c if mine else 1 - c]
        return remote(ref, ref, os_.at[delta - 1], or_.at[delta - 1], core_to)

    def r_send(delta):
        ref = resid.at[j]
        return remote(ref, ref, rs.at[delta - 1], rr.at[delta - 1], {"tp": tp_at(delta)})

    def r_recv(delta):
        ref = resid.at[tp_at(-delta)]
        return remote(ref, ref, rs.at[delta - 1], rr.at[delta - 1], {"tp": tp_at(delta)})

    def a_send(kind, delta):
        ref = att.at[j, kind]
        return remote(ref, ref, as_.at[kind, delta - 1], ar.at[kind, delta - 1], {"tp": tp_at(delta)})

    def a_recv(kind, delta):
        ref = att.at[tp_at(-delta), kind]
        return remote(ref, ref, as_.at[kind, delta - 1], ar.at[kind, delta - 1], {"tp": tp_at(delta)})

    def m_send(delta, o):
        src = part.at[o, pl.ds(pl.multiple_of(own_rows * tp_at(delta), own_rows), own_rows)]
        dst = mix.at[delta - 1, o]
        return remote(src, dst, ms.at[delta - 1, o], mr.at[delta - 1, o], {"tp": tp_at(delta)})

    def takes(kind, d, t):
        return t <= (half if LAST_WAY[kind] == d else half - 1)

    def passes(kind, d, t):
        return t <= (half - 1 if LAST_WAY[kind] == d else half - 2)

    def when(condition, run):
        if isinstance(condition, bool):
            if condition:
                run()
        else:
            pl.when(condition)(run)

    barrier = pltpu.get_barrier_semaphore()
    friends = [z_to[0], z_to[1], core_to, y_to] + [{"tp": tp_at(k)} for k in range(1, ntp)]
    for friend in friends:
        pl.semaphore_signal(barrier, inc=1, device_id=friend, device_id_type=MESH)
    kd = kv.shape[3]
    local = [
        pltpu.make_async_copy(src, dst, ls.at[i])
        for i, (src, dst) in enumerate(
            [
                (kn_ref, kv.at[s, 0]),
                (vn_ref, kv.at[s, 1]),
                (kw_ref.at[:, pl.ds(0, kd)], kv.at[s, 2]),
                (kw_ref.at[:, pl.ds(kd, kd)], kv.at[s, 3]),
                (vw_ref, kv.at[s, 4]),
                (up_ref, up.at[s]),
                (dn_ref, dn.at[s]),
                (on_ref, outs.at[j, 0]),
                (ow_ref, outs.at[j, 1]),
                (res_ref, resid.at[j]),
            ]
        )
    ]
    for copy in local:
        copy.start()
    acc[...] = jnp.zeros_like(acc)
    top[...] = jnp.full_like(top, -jnp.inf)
    pl.semaphore_wait(barrier, len(friends))
    for copy in local:
        copy.wait()
    for kind in (KV_N, KV_W, UP):
        for d in range(2):
            z_send(kind, d, 0).start()
        core_send((C_KV_N, C_KV_W, C_UP)[kind], 0, 0).start()
    for d in range(2):
        x_send(d).start()
    for delta in range(1, ntp):
        r_send(delta).start()
    core_send(C_DN, 0, 0).start()

    def pump(kind, t):
        for d in range(2):

            def arrived(d=d):
                z_recv(kind, d, t).wait_recv()

                def forward():
                    z_send(kind, d, t).start()

                when(passes(kind, d, t), forward)
                if kind in (KV_N, KV_W):
                    core_send((C_KV_N, C_KV_W)[kind], d, t).start()
                if kind == UP:
                    y_send(Y_UP, d, t).start()
                if kind == DN_B:
                    y_send(Y_DN, d, t).start()

            when(takes(kind, d, t), arrived)

    def complete(y_kind, core_kind, kind, t):
        for d in range(2):

            def done(d=d):
                y_recv(y_kind, d, t).wait_recv()
                core_send(core_kind, d, t).start()

            when(takes(kind, d, t), done)

    ones = jnp.ones((2 * rows, acc.shape[2] - kd), BF16)

    def attend(unit, chip):
        scale = widths[unit] ** -0.5 * LOG2E
        keys = kv[pl.ds(2 * chip, 2), KEY_PART[unit]].reshape(2 * rows, kd)
        values = kv[pl.ds(2 * chip, 2), VALUE_PART[unit]].reshape(2 * rows, kd)
        values = jnp.concatenate([values, ones], axis=1)
        lanes = top.shape[2]
        for row in range(0, q_ref.shape[1], Q_TILE):
            tile = pl.ds(row, Q_TILE)
            scores = lax.dot_general(
                q_ref[unit, tile], keys, (((1,), (1,)), ((), ())), preferred_element_type=F32
            )
            old = top[unit, tile]
            new = jnp.maximum(old, jnp.max(scores, axis=1, keepdims=True))
            rescale = jnp.exp2((old - new) * scale)
            top[unit, tile] = new
            wide = jnp.concatenate([new] * (2 * rows // lanes), axis=1)
            powers = jnp.exp2((scores - wide) * scale).astype(BF16)
            weighted = jnp.dot(powers, values, preferred_element_type=F32)
            wide = jnp.concatenate([rescale] * (acc.shape[2] // lanes), axis=1)
            acc[unit, tile] = acc[unit, tile] * wide + weighted

    def step(t, _):
        dt = t - 1
        chips = jnp.where((dt == 0) | (dt == half), 1, 2)

        def over(units, core_kind):
            def one(i, _):
                chip = lax.rem(jnp.where(i == 0, z - dt, z + dt) + nz, nz)
                if core_kind is not None:
                    way = jnp.where(dt == half, CORE_LAST[core_kind], i)
                    core_recv(core_kind, way, dt, chip).wait_recv()
                for unit in units:
                    attend(unit, chip)
                return 0

            lax.fori_loop(0, chips, one, 0)

        more = t <= half
        over((0, 1), C_KV_N)
        pl.when(more)(lambda: pump(KV_N, t))
        over((2,), C_KV_W)
        pl.when(more)(lambda: pump(KV_W, t))
        over((3,), None)
        pl.when(more)(lambda: pump(UP, t))

        @pl.when(dt >= 1)
        def _():
            complete(Y_UP, C_UP, UP, dt)

        @pl.when(t == half // 2)
        def _():
            for d in range(2):
                x_recv(d).wait_recv()
                x_relay(d).start()

        @pl.when(t == half - 1)
        def _():
            for d in range(2):
                x_relayed(d).wait_recv()
            for delta in range(1, ntp):
                o_core(delta, True).start()

        @pl.when(t == half)
        def _():
            for kind in (DN_A, DN_B):
                for d in range(2):
                    z_send(kind, d, 0).start()

        return 0

    lax.fori_loop(1, half + 2, step, 0)

    def head_group(kind, lam_ref):
        for h in range(2):
            tile = pl.ds(h * rows, rows)
            one = acc[2 * kind, tile]
            two = acc[2 * kind + 1, tile]
            diff = one[:, :kd] / one[:, kd:] - lam_ref[h] * (two[:, :kd] / two[:, kd:])
            square = jnp.mean(diff * diff, axis=-1, keepdims=True)
            diff = diff * lax.rsqrt(square + NORM_EPS) * head_gain_ref[...] * OUT_SCALE
            att[j, kind, :, pl.ds(h * kd, kd)] = diff.astype(BF16)

    head_group(0, lam_n_ref)
    head_group(1, lam_w_ref)
    for kind in range(2):
        for delta in range(1, ntp):
            a_send(kind, delta).start()
    for t in range(1, 4):
        pump(DN_A, t)
        pump(DN_B, t)
        if t > 1:
            complete(Y_DN, C_DN, DN_B, t - 1)
    for delta in range(1, ntp):
        o_core(delta, False).wait_recv()
        r_recv(delta).wait_recv()
        for kind in range(2):
            a_recv(kind, delta).wait_recv()

    sumsq[...] = jnp.zeros_like(sumsq)
    width = mid.shape[1]

    def project(n, _):
        cols = pl.ds(pl.multiple_of(n * COLS, COLS), COLS)
        total = resid[:, :, cols].reshape(mid.shape[0], COLS).astype(F32)
        terms = jnp.zeros((mid.shape[0], COLS), F32)
        for peer in range(ntp):
            term = jnp.dot(att[peer, 0], outs[peer, 0, :, cols], preferred_element_type=F32)
            term = term + jnp.dot(att[peer, 1], outs[peer, 1, :, cols], preferred_element_type=F32)
            terms = terms + term.astype(BF16).astype(F32)
        total = (total + terms).astype(BF16)
        mid[:, cols] = total
        total = total.astype(F32)
        sumsq[...] += jnp.sum(total * total, axis=1, keepdims=True)
        return 0

    lax.fori_loop(0, width // COLS, project, 0)
    pump(DN_A, 4)
    pump(DN_B, 4)
    complete(Y_DN, C_DN, DN_B, 3)

    inverse = lax.rsqrt(sumsq[:, 0:1] * (1.0 / width) + NORM_EPS)

    def normalise(n, _):
        cols = pl.ds(pl.multiple_of(n * COLS, COLS), COLS)
        scaled = mid[:, cols].astype(F32) * inverse
        nrm[:, cols] = (scaled * norm_gain_ref[:, cols].astype(F32)).astype(BF16)
        return 0

    lax.fori_loop(0, width // COLS, normalise, 0)

    def up_wait(t, _):
        for d in range(2):

            def here(d=d):
                core_recv(C_UP, d, t, chip_at(d, t)).wait_recv()

            if d == 0:
                pl.when(t <= half - 1)(here)
            else:
                pl.when(t >= 1)(here)
        return 0

    lax.fori_loop(0, half + 1, up_wait, 0)

    def lift(n, _):
        cols = pl.ds(pl.multiple_of(n * COLS, COLS), COLS)
        weights = up[:, :, cols].reshape(width, COLS)
        lifted = jnp.dot(nrm[...], weights, preferred_element_type=F32)
        lifted = jnp.maximum(lifted, 0.0)
        act[:, cols] = (lifted * lifted).astype(BF16)
        return 0

    lift_steps = act.shape[1] // COLS
    lax.fori_loop(0, lift_steps // 2, lift, 0)
    pump(DN_A, 5)
    pump(DN_B, 5)
    complete(Y_DN, C_DN, DN_B, 4)
    lax.fori_loop(lift_steps // 2, lift_steps, lift, 0)

    def lower(o, t, chip, d):
        core_recv(C_DN, d, t, chip).wait_recv()
        weights = dn[pl.ds(2 * chip, 2)].reshape(2 * wrows, dn.shape[2])
        lowered = lax.dot_general(
            act[...], weights, (((1,), (1,)), ((), ())), preferred_element_type=F32
        )
        part[o] = lowered.astype(BF16)

    def lower_step(t):
        if t == 0:
            lower(0, 0, z, 0)
            done = (0,)
        elif t == half:
            lower(2 * half - 1, half, chip_at(1, half), 1)
            done = (2 * half - 1,)
        else:
            lower(2 * t - 1, t, chip_at(0, t), 0)
            lower(2 * t, t, chip_at(1, t), 1)
            done = (2 * t - 1, 2 * t)
        for o in done:
            for delta in range(1, ntp):
                m_send(delta, o).start()

    for t in range(0, half + 1):
        if t + 6 <= half:
            pump(DN_A, t + 6)
            pump(DN_B, t + 6)
        if t + 5 <= half:
            complete(Y_DN, C_DN, DN_B, t + 5)
        lower_step(t)

    own = pl.ds(pl.multiple_of(own_rows * j, own_rows), own_rows)

    def finish(o, _):
        t = (o + 1) // 2
        chip = lax.rem(jnp.where(o % 2 == 1, z - t, z + t) + nz, nz)
        cols = pl.ds(pl.multiple_of(chip * 2 * wrows, 2 * wrows), 2 * wrows)
        total = part[o, own].astype(F32)
        for delta in range(1, ntp):
            m_send(delta, o).wait_recv()
            total = total + mix[delta - 1, o].astype(F32)
        out_ref[:, cols] = (mid[own, cols].astype(F32) + total).astype(BF16)
        return 0

    lax.fori_loop(0, nz, finish, 0)

    def sent(t, _):
        for kind in range(5):
            for d in range(2):
                pl.when(passes(kind, d, t))(lambda kind=kind, d=d: z_send(kind, d, t).wait_send())
        for kind in range(4):
            for d in range(2):
                last = half if CORE_LAST[kind] == d else half - 1
                first = d
                pl.when((t >= first) & (t <= last))(
                    lambda kind=kind, d=d: core_send(kind, d, t).wait_send()
                )
        for kind in range(2):
            for d in range(2):
                last = half if d == 1 else half - 1
                pl.when((t >= 1) & (t <= last))(
                    lambda kind=kind, d=d: y_send(kind, d, t).wait_send()
                )
        return 0

    lax.fori_loop(0, half + 1, sent, 0)
    for d in range(2):
        x_send(d).wait_send()
        x_relay(d).wait_send()
    for delta in range(1, ntp):
        o_core(delta, True).wait_send()
        r_send(delta).wait_send()
        for kind in range(2):
            a_send(kind, delta).wait_send()

    def mix_sent(o, _):
        for delta in range(1, ntp):
            m_send(delta, o).wait_send()
        return 0

    lax.fori_loop(0, nz, mix_sent, 0)


def shards(
    nsp, ntp,
    resid_in, query_narrow, key_narrow, value_narrow, query_wide, key_wide, value_wide,
    lambda_narrow, lambda_wide, head_gain, out_narrow, out_wide, norm_gain, up_weight, down_weight,
):
    rows, heads, full = query_narrow.shape
    narrow, wide = full // 2, query_wide.shape[2] // 2
    width = resid_in.shape[1]
    hidden = up_weight.shape[1]
    qn = jnp.swapaxes(query_narrow, 0, 1).reshape(heads * rows, full)
    blank = jnp.zeros((heads * rows, narrow), BF16)
    qw = jnp.swapaxes(query_wide, 0, 1).reshape(heads * rows, 2 * wide)
    queries = jnp.stack(
        [
            jnp.concatenate([qn[:, :narrow], blank], axis=1),
            jnp.concatenate([blank, qn[:, narrow:]], axis=1),
            qw[:, :wide],
            qw[:, wide:],
        ]
    )
    nz = nsp // 2
    half = nz // 2
    anywhere = pl.BlockSpec(memory_space=pl.ANY)
    vmem = pl.BlockSpec(memory_space=pltpu.VMEM)
    smem = pl.BlockSpec(memory_space=pltpu.SMEM)
    dma = pltpu.SemaphoreType.DMA
    own_rows = resid_in.shape[0]
    out_rows = out_narrow.shape[0]
    down = down_weight.T
    return pl.pallas_call(
        functools.partial(layer_kernel, nz, ntp, (narrow, narrow, wide, wide)),
        out_shape=jax.ShapeDtypeStruct(resid_in.shape, BF16),
        in_specs=[vmem] + [anywhere] * 9 + [smem, smem, vmem, vmem],
        out_specs=vmem,
        scratch_shapes=[
            pltpu.VMEM((nsp, 5, rows, wide), BF16),
            pltpu.VMEM((nsp, up_weight.shape[0], hidden), BF16),
            pltpu.VMEM((nsp, down.shape[0], hidden), BF16),
            pltpu.VMEM((ntp, 2, out_rows, width), BF16),
            pltpu.VMEM((ntp, own_rows, width), BF16),
            pltpu.VMEM((4, heads * rows, 2 * wide), F32),
            pltpu.VMEM((4, heads * rows, 128), F32),
            pltpu.VMEM((ntp, 2, rows, out_rows), BF16),
            pltpu.VMEM((rows, width), BF16),
            pltpu.VMEM((rows, width), BF16),
            pltpu.VMEM((rows, hidden), BF16),
            pltpu.VMEM((nz, rows, 2 * down.shape[0]), BF16),
            pltpu.VMEM((ntp - 1, nz, own_rows, 2 * down.shape[0]), BF16),
            pltpu.VMEM((rows, 128), F32),
            dma((5, 2, half)),
            dma((5, 2, half + 1)),
            dma((4, 2, half + 1)),
            dma((4, 2, half + 1)),
            dma((2, 2, half + 1)),
            dma((2, 2, half + 1)),
            dma((4,)),
            dma((4,)),
            dma((ntp - 1,)),
            dma((ntp - 1,)),
            dma((ntp - 1,)),
            dma((ntp - 1,)),
            dma((2, ntp - 1)),
            dma((2, ntp - 1)),
            dma((ntp - 1, nz)),
            dma((ntp - 1, nz)),
            dma((10,)),
        ],
        compiler_params=pltpu.CompilerParams(
            collective_id=0, has_side_effects=True, vmem_limit_bytes=62 * 1024 * 1024
        ),
        name="layer",
    )(
        queries,
        key_narrow.reshape(rows, full),
        value_narrow.reshape(rows, -1),
        key_wide.reshape(rows, 2 * wide),
        value_wide.reshape(rows, -1),
        up_weight,
        down,
        out_narrow,
        out_wide,
        resid_in,
        lambda_narrow,
        lambda_wide,
        head_gain.reshape(1, -1),
        norm_gain.reshape(1, -1),
    )


def solution(mesh):
    placed = (
        P(("grp", "sp", "tp"), None),
        P(("grp", "sp"), "tp", None),
        P(("grp", "sp"), "tp", None),
        P(("grp", "sp"), "tp", None),
        P(("grp", "sp"), "tp", None),
        P(("grp", "sp"), "tp", None),
        P(("grp", "sp"), "tp", None),
        P("tp"),
        P("tp"),
        P(),
        P("tp", None),
        P("tp", None),
        P(),
        P("sp", "tp"),
        P("tp", "sp"),
    )
    return jax.shard_map(
        functools.partial(shards, mesh.shape["sp"], mesh.shape["tp"]),
        mesh=mesh,
        in_specs=placed,
        out_specs=P(("grp", "sp", "tp"), None),
        check_vma=False,
    )
```

```python
import functools
import math

import jax
import jax.numpy as jnp
from jax import lax
from jax.experimental import pallas as pl
from jax.experimental.pallas import tpu as pltpu
from jax.sharding import PartitionSpec as P

NORM_EPS = 1e-06
OUT_SCALE = 0.8
LOG2E = math.log2(math.e)
MESH = pl.DeviceIdType.MESH
BF16 = jnp.bfloat16
F32 = jnp.float32

KV_N, KV_W, UP, DN_1, DN_2, DN_Y = range(6)
LAST_WAY = (1, 0, 1, 0, 1, 1)
C_KV_N, C_KV_W, C_DN, C_UP = range(4)
CORE_LAST = (1, 0, 1, 1)
Y_UP, Y_DN = range(2)
KEY_PART = (0, 0, 2, 3)
VALUE_PART = (1, 1, 4, 4)
Q_TILE = 128
COLS = 512
GROUPS = ((0, 1, 2), (3, 4), (5, 6), (7,), (8,))


def layer_kernel(
    nz, ntp, widths,
    qn_ref, qw_ref, kn_ref, vn_ref, kw_ref, vw_ref, up_ref, dn_ref, on_ref, ow_ref, res_ref,
    lam_n_ref, lam_w_ref, head_gain_ref, norm_gain_ref,
    out_ref,
    q, kv, up, dn, outs, resid, acc, top, att, mid, nrm, act, part, mix, sumsq,
    zs, zr, cs, cr, cu, ys, yr, xs, xr, os_, or_, rs, rr, as_, ar, ms, mr, ls,
):
    g, s, j = lax.axis_index("grp"), lax.axis_index("sp"), lax.axis_index("tp")
    z, c = s // 2, s % 2
    par = g % 2
    half = nz // 2
    rows = kv.shape[2]
    wrows = up.shape[1]
    hrows = wrows // 2
    qrows = wrows // 4
    own_rows = resid.shape[1]

    def sp_of(chip):
        return {"sp": 2 * lax.rem(chip + nz, nz) + c}

    z_to = (sp_of(z + 1), sp_of(z - 1))
    core_to = {"sp": 2 * z + 1 - c}
    y_to = {"grp": g + 1 - 2 * par}

    def tp_at(delta):
        return lax.rem(j + delta + ntp, ntp)

    def chip_at(d, t):
        return lax.rem(z - t + nz, nz) if d == 0 else lax.rem(z + t, nz)

    def slot(d, t):
        if isinstance(t, int) and isinstance(d, int):
            return 0 if t == 0 else 2 * half - 1 if t == half else 2 * t - 1 + d
        return jnp.where(t == 0, 0, jnp.where(t == half, 2 * half - 1, 2 * t - 1 + d))

    def piece(kind, block):
        if kind == KV_N:
            return kv.at[block, pl.ds(0, 2)]
        if kind == KV_W:
            return kv.at[block, pl.ds(2, 3)]
        if kind == UP:
            return up.at[block, pl.ds(pl.multiple_of(hrows * par, hrows), hrows)]
        if kind in (DN_1, DN_2):
            return dn.at[block, pl.ds(qrows * (1 + kind - DN_1), qrows)]
        return dn.at[block, pl.ds(pl.multiple_of(3 * qrows * par, qrows), qrows)]

    def remote(src, dst, send, recv, to):
        return pltpu.make_async_remote_copy(src, dst, send, recv, device_id=to, device_id_type=MESH)

    def z_send(kind, d, t):
        ref = piece(kind, 2 * chip_at(d, t) + c)
        return remote(ref, ref, zs.at[kind], zr.at[kind, slot(d, t + 1) - 1], z_to[d])

    def z_recv(kind, d, t):
        ref = piece(kind, 2 * chip_at(d, t) + c)
        return remote(ref, ref, zs.at[kind], zr.at[kind, slot(d, t) - 1], z_to[d])

    def core_piece(kind, block):
        if kind == C_KV_N:
            return kv.at[block, pl.ds(0, 2)]
        if kind == C_KV_W:
            return kv.at[block, pl.ds(2, 3)]
        return (up if kind == C_UP else dn).at[block]

    def core_got(kind, d, t):
        return cu.at[0] if kind == C_UP else cr.at[kind, slot(d, t)]

    def core_send(kind, d, t):
        ref = core_piece(kind, 2 * chip_at(d, t) + c)
        return remote(ref, ref, cs.at[kind], core_got(kind, d, t), core_to)

    def core_recv(kind, d, t, chip):
        ref = core_piece(kind, 2 * chip + 1 - c)
        return remote(ref, ref, cs.at[kind], core_got(kind, d, t), core_to)

    def y_piece(kind, block, side):
        if kind == Y_UP:
            return up.at[block, pl.ds(pl.multiple_of(hrows * side, hrows), hrows)]
        return dn.at[block, pl.ds(pl.multiple_of(3 * qrows * side, qrows), qrows)]

    def y_send(kind, d, t):
        ref = y_piece(kind, 2 * chip_at(d, t) + c, par)
        return remote(ref, ref, ys.at[kind], yr.at[kind, slot(d, t) - 1], y_to)

    def y_recv(kind, d, t):
        ref = y_piece(kind, 2 * chip_at(d, t) + c, 1 - par)
        return remote(ref, ref, ys.at[kind], yr.at[kind, slot(d, t) - 1], y_to)

    def x_send(d):
        ref = outs.at[j, c]
        return remote(ref, ref, xs.at[d], xr.at[d], {"tp": tp_at(1 - 2 * d)})

    def x_recv(d):
        ref = outs.at[tp_at(2 * d - 1), c]
        return remote(ref, ref, xs.at[d], xr.at[d], {"tp": tp_at(1 - 2 * d)})

    def x_half(owner, d):
        n = outs.shape[2] // 2
        return outs.at[owner, c, pl.ds(n * d, n)]

    def x_relay(d):
        ref = x_half(tp_at(2 * d - 1), d)
        return remote(ref, ref, xs.at[2 + d], xr.at[2 + d], {"tp": tp_at(1 - 2 * d)})

    def x_relayed(d):
        ref = x_half(tp_at(2), d)
        return remote(ref, ref, xs.at[2 + d], xr.at[2 + d], {"tp": tp_at(1 - 2 * d)})

    def o_core(delta, mine):
        ref = outs.at[tp_at(delta), c if mine else 1 - c]
        return remote(ref, ref, os_.at[0], or_.at[0], core_to)

    def r_send(delta):
        ref = resid.at[j]
        return remote(ref, ref, rs.at[0], rr.at[0], {"tp": tp_at(delta)})

    def r_recv(delta):
        ref = resid.at[tp_at(-delta)]
        return remote(ref, ref, rs.at[0], rr.at[0], {"tp": tp_at(delta)})

    def a_send(kind, delta):
        ref = att.at[j, kind]
        return remote(ref, ref, as_.at[0], ar.at[0], {"tp": tp_at(delta)})

    def a_recv(kind, delta):
        ref = att.at[tp_at(-delta), kind]
        return remote(ref, ref, as_.at[0], ar.at[0], {"tp": tp_at(delta)})

    def m_send(delta, group):
        first = max(2 * GROUPS[group][0] - 1, 0)
        count = min(2 * GROUPS[group][-1], nz - 1) + 1 - first
        rows_to = pl.ds(pl.multiple_of(own_rows * tp_at(delta), own_rows), own_rows)
        src = part.at[pl.ds(first, count), rows_to]
        dst = mix.at[delta - 1, pl.ds(first, count)]
        return remote(src, dst, ms.at[0], mr.at[delta - 1, group], {"tp": tp_at(delta)})

    def all_of(ref, send, recv):
        return remote(ref, ref, send, recv, core_to)

    def takes(kind, d, t):
        return t <= (half if LAST_WAY[kind] == d else half - 1)

    def passes(kind, d, t):
        return t <= (half - 1 if LAST_WAY[kind] == d else half - 2)

    def when(condition, run):
        if isinstance(condition, bool):
            if condition:
                run()
        else:
            pl.when(condition)(run)

    barrier = pltpu.get_barrier_semaphore()
    friends = [z_to[0], z_to[1], core_to, y_to] + [{"tp": tp_at(k)} for k in range(1, ntp)]
    for friend in friends:
        pl.semaphore_signal(barrier, inc=1, device_id=friend, device_id_type=MESH)
    kd = kv.shape[3]
    local = [
        pltpu.make_async_copy(src, dst, ls.at[i])
        for src, dst, i in [
            (kn_ref, kv.at[s, 0], 0),
            (vn_ref, kv.at[s, 1], 0),
            (kw_ref.at[:, pl.ds(0, kd)], kv.at[s, 2], 0),
            (kw_ref.at[:, pl.ds(kd, kd)], kv.at[s, 3], 0),
            (vw_ref, kv.at[s, 4], 0),
            (up_ref, up.at[s], 1),
            (on_ref, outs.at[j, 0], 2),
            (ow_ref, outs.at[j, 1], 2),
            (res_ref, resid.at[j], 3),
            (dn_ref, dn.at[s], 4),
        ]
    ]
    for copy in local:
        copy.start()

    def local_wait(ref, i):
        pltpu.make_async_copy(ref, ref, ls.at[i]).wait()

    pl.semaphore_wait(barrier, len(friends))
    local_wait(kv.at[s], 0)
    for kind in (KV_N, KV_W):
        for d in range(2):
            z_send(kind, d, 0).start()
        core_send((C_KV_N, C_KV_W)[kind], 0, 0).start()
    local_wait(up.at[s], 1)
    for d in range(2):
        z_send(UP, d, 0).start()
    core_send(C_UP, 0, 0).start()
    local_wait(outs.at[j], 2)
    for d in range(2):
        x_send(d).start()
    local_wait(resid.at[j], 3)
    for delta in range(1, ntp):
        r_send(delta).start()
    local_wait(dn.at[s], 4)
    core_send(C_DN, 0, 0).start()

    acc[...] = jnp.zeros_like(acc)
    top[...] = jnp.full_like(top, -jnp.inf)
    narrow_q = qn_ref[...].astype(F32)
    first_map = lax.broadcasted_iota(jnp.int32, narrow_q.shape, 1) < kd // 2
    q[0] = jnp.where(first_map, narrow_q, 0.0).astype(BF16)
    q[1] = jnp.where(first_map, 0.0, narrow_q).astype(BF16)
    q[2] = qw_ref[:, :kd]
    q[3] = qw_ref[:, kd:]

    def pump(kind, t):
        for d in range(2):

            def arrived(d=d):
                z_recv(kind, d, t).wait_recv()

                def forward():
                    z_send(kind, d, t).start()

                when(passes(kind, d, t), forward)
                if kind in (KV_N, KV_W):
                    core_send((C_KV_N, C_KV_W)[kind], d, t).start()
                if kind == UP:
                    y_send(Y_UP, d, t).start()
                if kind == DN_Y:
                    y_send(Y_DN, d, t).start()

            when(takes(kind, d, t), arrived)

    def complete(y_kind, core_kind, kind, t):
        for d in range(2):

            def done(d=d):
                y_recv(y_kind, d, t).wait_recv()
                core_send(core_kind, d, t).start()

            when(takes(kind, d, t), done)

    ones = jnp.ones((2 * rows, acc.shape[2] - kd), BF16)

    def attend(unit, chip):
        scale = widths[unit] ** -0.5 * LOG2E
        keys = kv[pl.ds(2 * chip, 2), KEY_PART[unit]].reshape(2 * rows, kd)
        values = kv[pl.ds(2 * chip, 2), VALUE_PART[unit]].reshape(2 * rows, kd)
        values = jnp.concatenate([values, ones], axis=1)
        lanes = top.shape[2]
        for row in range(0, q.shape[1], Q_TILE):
            tile = pl.ds(row, Q_TILE)
            scores = lax.dot_general(
                q[unit, tile], keys, (((1,), (1,)), ((), ())), preferred_element_type=F32
            )
            old = top[unit, tile]
            new = jnp.maximum(old, jnp.max(scores, axis=1, keepdims=True))
            rescale = jnp.exp2((old - new) * scale)
            top[unit, tile] = new
            wide = jnp.concatenate([new] * (2 * rows // lanes), axis=1)
            powers = jnp.exp2((scores - wide) * scale).astype(BF16)
            weighted = jnp.dot(powers, values, preferred_element_type=F32)
            wide = jnp.concatenate([rescale] * (acc.shape[2] // lanes), axis=1)
            acc[unit, tile] = acc[unit, tile] * wide + weighted

    def head_group(kind, lam_ref):
        for h in range(2):
            tile = pl.ds(h * rows, rows)
            one = acc[2 * kind, tile]
            two = acc[2 * kind + 1, tile]
            diff = one[:, :kd] / one[:, kd:] - lam_ref[h] * (two[:, :kd] / two[:, kd:])
            square = jnp.mean(diff * diff, axis=-1, keepdims=True)
            diff = diff * lax.rsqrt(square + NORM_EPS) * head_gain_ref[...] * OUT_SCALE
            att[j, kind, :, pl.ds(h * kd, kd)] = diff.astype(BF16)

    def step(t, _):
        dt = t - 1
        chips = jnp.where((dt == 0) | (dt == half), 1, 2)

        def over(units, core_kind):
            def one(i, _):
                chip = lax.rem(jnp.where(i == 0, z - dt, z + dt) + nz, nz)
                if core_kind is not None:
                    way = jnp.where(dt == half, CORE_LAST[core_kind], i)
                    core_recv(core_kind, way, dt, chip).wait_recv()
                for unit in units:
                    attend(unit, chip)
                return 0

            lax.fori_loop(0, chips, one, 0)

        more = t <= half
        over((0, 1), C_KV_N)
        pl.when(more)(lambda: pump(KV_N, t))

        @pl.when(t == half + 1)
        def _():
            pump(DN_1, 1)
            head_group(0, lam_n_ref)
            for delta in range(1, ntp):
                a_send(0, delta).start()

        over((2,), C_KV_W)
        pl.when(more)(lambda: pump(KV_W, t))
        pl.when(t == half + 1)(lambda: pump(DN_2, 1))
        over((3,), None)
        pl.when(more)(lambda: pump(UP, t))
        pl.when(t == half + 1)(lambda: pump(DN_Y, 1))

        @pl.when(t == half - 1)
        def _():
            for kind in (DN_1, DN_2, DN_Y):
                for d in range(2):
                    z_send(kind, d, 0).start()

        @pl.when(dt >= 1)
        def _():
            complete(Y_UP, C_UP, UP, dt)

        @pl.when(t == half // 2)
        def _():
            for d in range(2):
                x_recv(d).wait_recv()
                x_relay(d).start()
            o_core(1, True).start()

        pl.when(t == half // 2 + 1)(lambda: o_core(ntp - 1, True).start())

        @pl.when(t == half - 2)
        def _():
            for d in range(2):
                x_relayed(d).wait_recv()
            o_core(2, True).start()

        return 0

    lax.fori_loop(1, half + 2, step, 0)

    head_group(1, lam_w_ref)
    for delta in range(1, ntp):
        a_send(1, delta).start()

    relays = [(kind, t) for t in range(2, half + 1) for kind in (DN_1, DN_2, DN_Y)]

    def relay(count):
        for _ in range(min(count, len(relays))):
            kind, t = relays.pop(0)
            pump(kind, t)
            if kind == DN_Y:
                complete(Y_DN, C_DN, DN_Y, t - 1)

    relay(6)
    all_of(outs.at[pl.ds(0, ntp - 1), 0], os_.at[0], or_.at[0]).wait_recv()
    all_of(resid.at[pl.ds(0, ntp - 1)], rs.at[0], rr.at[0]).wait_recv()
    all_of(att.at[pl.ds(0, ntp - 1)], as_.at[0], ar.at[0]).wait_recv()

    width = mid.shape[1]
    squares = jnp.zeros((mid.shape[0], 128), F32)
    for n in range(0, width, COLS):
        cols = pl.ds(n, COLS)
        total = resid[:, :, cols].reshape(mid.shape[0], COLS).astype(F32)
        terms = jnp.zeros((mid.shape[0], COLS), F32)
        for peer in range(ntp):
            term = jnp.dot(att[peer, 0], outs[peer, 0, :, cols], preferred_element_type=F32)
            term = term + jnp.dot(att[peer, 1], outs[peer, 1, :, cols], preferred_element_type=F32)
            terms = terms + term.astype(BF16).astype(F32)
        total = (total + terms).astype(BF16)
        mid[:, cols] = total
        total = total.astype(F32)
        total = total * total
        for k in range(0, COLS, 128):
            squares = squares + total[:, k : k + 128]
        sumsq[...] = squares
        relay(1)
        squares = sumsq[...]

    inverse = lax.rsqrt(jnp.sum(squares, axis=1, keepdims=True) * (1.0 / width) + NORM_EPS)
    for k in range(width // 128):
        cols = pl.ds(128 * k, 128)
        gain = norm_gain_ref[k : k + 1, :].astype(F32)
        nrm[:, cols] = (mid[:, cols].astype(F32) * inverse * gain).astype(BF16)
    relay(1)

    all_of(up.at[pl.ds(0, nz)], cs.at[C_UP], cu.at[0]).wait_recv()
    for n in range(0, act.shape[1], COLS):
        cols = pl.ds(n, COLS)
        weights = up[:, :, cols].reshape(width, COLS)
        lifted = jnp.dot(nrm[...], weights, preferred_element_type=F32)
        lifted = jnp.maximum(lifted, 0.0)
        act[:, cols] = (lifted * lifted).astype(BF16)
        relay(1)

    def chips_of(t):
        if t in (0, half):
            return [(0 if t == 0 else 1, chip_at(1, t))]
        return [(d, chip_at(d, t)) for d in range(2)]

    def lower(t):
        weights = []
        for d, chip in chips_of(t):
            core_recv(C_DN, d, t, chip).wait_recv()
            weights.append(dn[pl.ds(2 * chip, 2)].reshape(2 * wrows, dn.shape[2]))
        weights = weights[0] if len(weights) == 1 else jnp.concatenate(weights, axis=0)
        lowered = lax.dot_general(
            act[...], weights, (((1,), (1,)), ((), ())), preferred_element_type=F32
        ).astype(BF16)
        for i in range(len(chips_of(t))):
            part[max(2 * t - 1, 0) + i] = lowered[:, 2 * wrows * i : 2 * wrows * (i + 1)]

    own = pl.ds(pl.multiple_of(own_rows * j, own_rows), own_rows)

    def finish(group):
        for delta in range(1, ntp):
            m_send(delta, group).wait_recv()
        for t in GROUPS[group]:
            for i, (_, chip) in enumerate(chips_of(t)):
                o = max(2 * t - 1, 0) + i
                cols = pl.ds(pl.multiple_of(chip * 2 * wrows, 2 * wrows), 2 * wrows)
                total = part[o, own].astype(F32)
                for delta in range(1, ntp):
                    total = total + mix[delta - 1, o].astype(F32)
                out_ref[:, cols] = (mid[own, cols].astype(F32) + total).astype(BF16)

    for group, distances in enumerate(GROUPS):
        for t in distances:
            lower(t)
            relay(1 if t < 4 else 2)
            if t == 5:
                complete(Y_DN, C_DN, DN_Y, half)
        for delta in range(1, ntp):
            m_send(delta, group).start()
        if group > 0:
            finish(group - 1)
    finish(len(GROUPS) - 1)

    blocks = nz - 1
    for kind in (KV_N, KV_W):
        parts = pl.ds(0, 2 if kind == KV_N else 3)
        all_of(kv.at[pl.ds(0, blocks), parts], zs.at[kind], cu.at[0]).wait_send()
        all_of(kv.at[pl.ds(0, nz), parts], cs.at[kind], cu.at[0]).wait_send()
    all_of(up.at[pl.ds(0, blocks), pl.ds(0, hrows)], zs.at[UP], cu.at[0]).wait_send()
    all_of(up.at[pl.ds(0, blocks), pl.ds(0, hrows)], ys.at[Y_UP], cu.at[0]).wait_send()
    for kind in (DN_1, DN_2, DN_Y):
        all_of(dn.at[pl.ds(0, blocks), pl.ds(0, qrows)], zs.at[kind], cu.at[0]).wait_send()
    all_of(dn.at[pl.ds(0, blocks), pl.ds(0, qrows)], ys.at[Y_DN], cu.at[0]).wait_send()
    all_of(up.at[pl.ds(0, nz)], cs.at[C_UP], cu.at[0]).wait_send()
    all_of(dn.at[pl.ds(0, nz)], cs.at[C_DN], cu.at[0]).wait_send()
    for d in range(2):
        x_send(d).wait_send()
        x_relay(d).wait_send()
    all_of(outs.at[pl.ds(0, ntp - 1), 0], os_.at[0], or_.at[0]).wait_send()
    all_of(resid.at[pl.ds(0, ntp - 1)], rs.at[0], rr.at[0]).wait_send()
    all_of(att.at[pl.ds(0, ntp - 1)], as_.at[0], ar.at[0]).wait_send()
    all_of(mix, ms.at[0], mr.at[0, 0]).wait_send()


def shards(
    nsp, ntp,
    resid_in, query_narrow, key_narrow, value_narrow, query_wide, key_wide, value_wide,
    lambda_narrow, lambda_wide, head_gain, out_narrow, out_wide, norm_gain, up_weight, down_weight,
):
    rows, heads, full = query_narrow.shape
    narrow, wide = full // 2, query_wide.shape[2] // 2
    width = resid_in.shape[1]
    hidden = up_weight.shape[1]
    qn = jnp.swapaxes(query_narrow, 0, 1).reshape(heads * rows, full)
    qw = jnp.swapaxes(query_wide, 0, 1).reshape(heads * rows, 2 * wide)
    nz = nsp // 2
    anywhere = pl.BlockSpec(memory_space=pl.ANY)
    vmem = pl.BlockSpec(memory_space=pltpu.VMEM)
    smem = pl.BlockSpec(memory_space=pltpu.SMEM)
    dma = pltpu.SemaphoreType.DMA
    own_rows = resid_in.shape[0]
    out_rows = out_narrow.shape[0]
    down = down_weight.T
    return pl.pallas_call(
        functools.partial(layer_kernel, nz, ntp, (narrow, narrow, wide, wide)),
        out_shape=jax.ShapeDtypeStruct(resid_in.shape, BF16),
        in_specs=[vmem, vmem] + [anywhere] * 9 + [smem, smem, vmem, vmem],
        out_specs=vmem,
        scratch_shapes=[
            pltpu.VMEM((4, heads * rows, wide), BF16),
            pltpu.VMEM((nsp, 5, rows, wide), BF16),
            pltpu.VMEM((nsp, up_weight.shape[0], hidden), BF16),
            pltpu.VMEM((nsp, down.shape[0], hidden), BF16),
            pltpu.VMEM((ntp, 2, out_rows, width), BF16),
            pltpu.VMEM((ntp, own_rows, width), BF16),
            pltpu.VMEM((4, heads * rows, 2 * wide), F32),
            pltpu.VMEM((4, heads * rows, 128), F32),
            pltpu.VMEM((ntp, 2, rows, out_rows), BF16),
            pltpu.VMEM((rows, width), BF16),
            pltpu.VMEM((rows, width), BF16),
            pltpu.VMEM((rows, hidden), BF16),
            pltpu.VMEM((nz, rows, 2 * down.shape[0]), BF16),
            pltpu.VMEM((ntp - 1, nz, own_rows, 2 * down.shape[0]), BF16),
            pltpu.VMEM((rows, 128), F32),
            dma((6,)),
            dma((6, nz - 1)),
            dma((4,)),
            dma((3, nz)),
            dma((1,)),
            dma((2,)),
            dma((2, nz - 1)),
            dma((4,)),
            dma((4,)),
            dma((1,)),
            dma((1,)),
            dma((1,)),
            dma((1,)),
            dma((1,)),
            dma((1,)),
            dma((1,)),
            dma((ntp - 1, len(GROUPS))),
            dma((5,)),
        ],
        compiler_params=pltpu.CompilerParams(
            collective_id=0, has_side_effects=True, vmem_limit_bytes=62 * 1024 * 1024
        ),
        name="layer",
    )(
        qn,
        qw,
        key_narrow.reshape(rows, full),
        value_narrow.reshape(rows, -1),
        key_wide.reshape(rows, 2 * wide),
        value_wide.reshape(rows, -1),
        up_weight,
        down,
        out_narrow,
        out_wide,
        resid_in,
        lambda_narrow,
        lambda_wide,
        head_gain.reshape(1, -1),
        norm_gain.reshape(-1, 128),
    )


def solution(mesh):
    placed = (
        P(("grp", "sp", "tp"), None),
        P(("grp", "sp"), "tp", None),
        P(("grp", "sp"), "tp", None),
        P(("grp", "sp"), "tp", None),
        P(("grp", "sp"), "tp", None),
        P(("grp", "sp"), "tp", None),
        P(("grp", "sp"), "tp", None),
        P("tp"),
        P("tp"),
        P(),
        P("tp", None),
        P("tp", None),
        P(),
        P("sp", "tp"),
        P("tp", "sp"),
    )
    return jax.shard_map(
        functools.partial(shards, mesh.shape["sp"], mesh.shape["tp"]),
        mesh=mesh,
        in_specs=placed,
        out_specs=P(("grp", "sp", "tp"), None),
        check_vma=False,
    )
```

```python
import functools
import math

import jax
import jax.numpy as jnp
from jax import lax
from jax.experimental import pallas as pl
from jax.experimental.pallas import tpu as pltpu
from jax.sharding import PartitionSpec as P

NORM_EPS = 1e-06
OUT_SCALE = 0.8
LOG2E = math.log2(math.e)
MESH = pl.DeviceIdType.MESH
BF16 = jnp.bfloat16
F32 = jnp.float32

KV_N, KV_W, UP, DN_Y, DN_1, DN_2 = range(6)
LAST_WAY = (1, 0, 1, 1, 0, 1)
C_KV_N, C_KV_W, C_DN, C_UP = range(4)
CORE_LAST = (1, 0, 1, 1)
Y_UP, Y_DN = range(2)
KEY_PART = (0, 0, 2, 3)
VALUE_PART = (1, 1, 4, 4)
Q_TILE = 128
COLS = 512
GROUPS = ((0, 1, 2), (3, 4), (5, 6), (7,), (8,))


def layer_kernel(
    nz, ntp, widths,
    qn_ref, qw_ref, kn_ref, vn_ref, kw_ref, vw_ref, up_ref, dn_ref, on_ref, ow_ref, res_ref,
    lam_n_ref, lam_w_ref, head_gain_ref, norm_gain_ref,
    out_ref,
    qn, qw, q, kv, up, dn, outs, resid, acc, top, att, mid, nrm, act, part, mix, sumsq,
    zs, zr, cs, cr, cu, ys, yr, xs, xr, os_, or_, rs, rr, as_, ar, ms, mr, ls,
):
    g, s, j = lax.axis_index("grp"), lax.axis_index("sp"), lax.axis_index("tp")
    z, c = s // 2, s % 2
    par = g % 2
    half = nz // 2
    rows = kv.shape[2]
    wrows = up.shape[1]
    hrows = wrows // 2
    qrows = wrows // 4
    own_rows = resid.shape[1]

    def sp_of(chip):
        return {"sp": 2 * lax.rem(chip + nz, nz) + c}

    z_to = (sp_of(z + 1), sp_of(z - 1))
    core_to = {"sp": 2 * z + 1 - c}
    y_to = {"grp": g + 1 - 2 * par}

    def tp_at(delta):
        return lax.rem(j + delta + ntp, ntp)

    def chip_at(d, t):
        return lax.rem(z - t + nz, nz) if d == 0 else lax.rem(z + t, nz)

    def slot(d, t):
        if isinstance(t, int) and isinstance(d, int):
            return 0 if t == 0 else 2 * half - 1 if t == half else 2 * t - 1 + d
        return jnp.where(t == 0, 0, jnp.where(t == half, 2 * half - 1, 2 * t - 1 + d))

    def piece(kind, block):
        if kind == KV_N:
            return kv.at[block, pl.ds(0, 2)]
        if kind == KV_W:
            return kv.at[block, pl.ds(2, 3)]
        if kind == UP:
            return up.at[block, pl.ds(pl.multiple_of(hrows * par, hrows), hrows)]
        if kind in (DN_1, DN_2):
            return dn.at[block, pl.ds(qrows * (1 + kind - DN_1), qrows)]
        return dn.at[block, pl.ds(pl.multiple_of(3 * qrows * par, qrows), qrows)]

    def remote(src, dst, send, recv, to):
        return pltpu.make_async_remote_copy(src, dst, send, recv, device_id=to, device_id_type=MESH)

    def z_send(kind, d, t):
        ref = piece(kind, 2 * chip_at(d, t) + c)
        return remote(ref, ref, zs.at[kind], zr.at[kind, slot(d, t + 1) - 1], z_to[d])

    def z_recv(kind, d, t):
        ref = piece(kind, 2 * chip_at(d, t) + c)
        return remote(ref, ref, zs.at[kind], zr.at[kind, slot(d, t) - 1], z_to[d])

    def core_piece(kind, block):
        if kind == C_KV_N:
            return kv.at[block, pl.ds(0, 2)]
        if kind == C_KV_W:
            return kv.at[block, pl.ds(2, 3)]
        return (up if kind == C_UP else dn).at[block]

    def core_got(kind, d, t):
        return cu.at[0] if kind == C_UP else cr.at[kind, slot(d, t)]

    def core_send(kind, d, t):
        ref = core_piece(kind, 2 * chip_at(d, t) + c)
        return remote(ref, ref, cs.at[kind], core_got(kind, d, t), core_to)

    def core_recv(kind, d, t, chip):
        ref = core_piece(kind, 2 * chip + 1 - c)
        return remote(ref, ref, cs.at[kind], core_got(kind, d, t), core_to)

    def y_piece(kind, block, side):
        if kind == Y_UP:
            return up.at[block, pl.ds(pl.multiple_of(hrows * side, hrows), hrows)]
        return dn.at[block, pl.ds(pl.multiple_of(3 * qrows * side, qrows), qrows)]

    def y_send(kind, d, t):
        ref = y_piece(kind, 2 * chip_at(d, t) + c, par)
        return remote(ref, ref, ys.at[kind], yr.at[kind, slot(d, t) - 1], y_to)

    def y_recv(kind, d, t):
        ref = y_piece(kind, 2 * chip_at(d, t) + c, 1 - par)
        return remote(ref, ref, ys.at[kind], yr.at[kind, slot(d, t) - 1], y_to)

    def x_send(d):
        ref = outs.at[j, c]
        return remote(ref, ref, xs.at[d], xr.at[d], {"tp": tp_at(1 - 2 * d)})

    def x_recv(d):
        ref = outs.at[tp_at(2 * d - 1), c]
        return remote(ref, ref, xs.at[d], xr.at[d], {"tp": tp_at(1 - 2 * d)})

    def x_half(owner, d):
        n = outs.shape[2] // 2
        return outs.at[owner, c, pl.ds(n * d, n)]

    def x_relay(d):
        ref = x_half(tp_at(2 * d - 1), d)
        return remote(ref, ref, xs.at[2 + d], xr.at[2 + d], {"tp": tp_at(1 - 2 * d)})

    def x_relayed(d):
        ref = x_half(tp_at(2), d)
        return remote(ref, ref, xs.at[2 + d], xr.at[2 + d], {"tp": tp_at(1 - 2 * d)})

    def o_core(delta, mine):
        ref = outs.at[tp_at(delta), c if mine else 1 - c]
        return remote(ref, ref, os_.at[0], or_.at[0], core_to)

    def r_send(delta):
        ref = resid.at[j]
        return remote(ref, ref, rs.at[0], rr.at[0], {"tp": tp_at(delta)})

    def r_recv(delta):
        ref = resid.at[tp_at(-delta)]
        return remote(ref, ref, rs.at[0], rr.at[0], {"tp": tp_at(delta)})

    def a_send(kind, delta):
        ref = att.at[j, kind]
        return remote(ref, ref, as_.at[0], ar.at[0], {"tp": tp_at(delta)})

    def a_recv(kind, delta):
        ref = att.at[tp_at(-delta), kind]
        return remote(ref, ref, as_.at[0], ar.at[0], {"tp": tp_at(delta)})

    def m_send(delta, group):
        first = max(2 * GROUPS[group][0] - 1, 0)
        count = min(2 * GROUPS[group][-1], nz - 1) + 1 - first
        rows_to = pl.ds(pl.multiple_of(own_rows * tp_at(delta), own_rows), own_rows)
        src = part.at[pl.ds(first, count), rows_to]
        dst = mix.at[delta - 1, pl.ds(first, count)]
        return remote(src, dst, ms.at[0], mr.at[delta - 1, group], {"tp": tp_at(delta)})

    def all_of(ref, send, recv):
        return remote(ref, ref, send, recv, core_to)

    def takes(kind, d, t):
        return t <= (half if LAST_WAY[kind] == d else half - 1)

    def passes(kind, d, t):
        return t <= (half - 1 if LAST_WAY[kind] == d else half - 2)

    def when(condition, run):
        if isinstance(condition, bool):
            if condition:
                run()
        else:
            pl.when(condition)(run)

    barrier = pltpu.get_barrier_semaphore()
    friends = [z_to[0], z_to[1], core_to, y_to] + [{"tp": tp_at(k)} for k in range(1, ntp)]
    for friend in friends:
        pl.semaphore_signal(barrier, inc=1, device_id=friend, device_id_type=MESH)
    kd = kv.shape[3]
    local = [
        pltpu.make_async_copy(src, dst, ls.at[i])
        for src, dst, i in [
            (kn_ref, kv.at[s, 0], 0),
            (vn_ref, kv.at[s, 1], 0),
            (kw_ref.at[:, pl.ds(0, kd)], kv.at[s, 2], 0),
            (kw_ref.at[:, pl.ds(kd, kd)], kv.at[s, 3], 0),
            (vw_ref, kv.at[s, 4], 0),
            (up_ref, up.at[s], 1),
            (on_ref, outs.at[j, 0], 2),
            (ow_ref, outs.at[j, 1], 2),
            (res_ref, resid.at[j], 3),
            (dn_ref, dn.at[s], 4),
            (qn_ref, qn, 5),
            (qw_ref, qw, 6),
        ]
    ]
    for copy in local:
        copy.start()

    def local_wait(ref, i):
        pltpu.make_async_copy(ref, ref, ls.at[i]).wait()

    pl.semaphore_wait(barrier, len(friends))
    local_wait(kv.at[s], 0)
    for kind in (KV_N, KV_W):
        for d in range(2):
            z_send(kind, d, 0).start()
        core_send((C_KV_N, C_KV_W)[kind], 0, 0).start()
    local_wait(up.at[s], 1)
    for d in range(2):
        z_send(UP, d, 0).start()
    core_send(C_UP, 0, 0).start()
    local_wait(outs.at[j], 2)
    for d in range(2):
        x_send(d).start()
    local_wait(resid.at[j], 3)
    for delta in range(1, ntp):
        r_send(delta).start()
    local_wait(dn.at[s], 4)
    core_send(C_DN, 0, 0).start()

    acc[...] = jnp.zeros_like(acc)
    top[...] = jnp.full_like(top, -jnp.inf)
    local_wait(qn, 5)
    local_wait(qw, 6)
    narrow_q = qn[...].astype(F32)
    wide_q = qw[...].astype(F32)
    first_map = lax.broadcasted_iota(jnp.int32, (rows, kd), 1) < kd // 2
    for h in range(2):
        tile = pl.ds(h * rows, rows)
        head = narrow_q[:, h, :]
        q[0, tile] = jnp.where(first_map, head, 0.0).astype(BF16)
        q[1, tile] = jnp.where(first_map, 0.0, head).astype(BF16)
        head = wide_q[:, h, :].astype(BF16)
        q[2, tile] = head[:, :kd]
        q[3, tile] = head[:, kd:]

    def pump(kind, t):
        for d in range(2):

            def arrived(d=d):
                z_recv(kind, d, t).wait_recv()

                def forward():
                    z_send(kind, d, t).start()

                when(passes(kind, d, t), forward)
                if kind in (KV_N, KV_W):
                    core_send((C_KV_N, C_KV_W)[kind], d, t).start()
                if kind == UP:
                    y_send(Y_UP, d, t).start()
                if kind == DN_Y:
                    y_send(Y_DN, d, t).start()

            when(takes(kind, d, t), arrived)

    def complete(y_kind, core_kind, kind, t):
        for d in range(2):

            def done(d=d):
                y_recv(y_kind, d, t).wait_recv()
                core_send(core_kind, d, t).start()

            when(takes(kind, d, t), done)

    ones = jnp.ones((2 * rows, acc.shape[2] - kd), BF16)

    def attend(unit, chip):
        scale = widths[unit] ** -0.5 * LOG2E
        keys = kv[pl.ds(2 * chip, 2), KEY_PART[unit]].reshape(2 * rows, kd)
        values = kv[pl.ds(2 * chip, 2), VALUE_PART[unit]].reshape(2 * rows, kd)
        values = jnp.concatenate([values, ones], axis=1)
        lanes = top.shape[2]
        for row in range(0, q.shape[1], Q_TILE):
            tile = pl.ds(row, Q_TILE)
            scores = lax.dot_general(
                q[unit, tile], keys, (((1,), (1,)), ((), ())), preferred_element_type=F32
            )
            old = top[unit, tile]
            new = jnp.maximum(old, jnp.max(scores, axis=1, keepdims=True))
            rescale = jnp.exp2((old - new) * scale)
            top[unit, tile] = new
            wide = jnp.concatenate([new] * (2 * rows // lanes), axis=1)
            powers = jnp.exp2((scores - wide) * scale).astype(BF16)
            weighted = jnp.dot(powers, values, preferred_element_type=F32)
            wide = jnp.concatenate([rescale] * (acc.shape[2] // lanes), axis=1)
            acc[unit, tile] = acc[unit, tile] * wide + weighted

    def head_group(kind, lam_ref):
        for h in range(2):
            tile = pl.ds(h * rows, rows)
            one = acc[2 * kind, tile]
            two = acc[2 * kind + 1, tile]
            diff = one[:, :kd] / one[:, kd:] - lam_ref[h] * (two[:, :kd] / two[:, kd:])
            square = jnp.mean(diff * diff, axis=-1, keepdims=True)
            diff = diff * lax.rsqrt(square + NORM_EPS) * head_gain_ref[...] * OUT_SCALE
            att[j, kind, :, pl.ds(h * kd, kd)] = diff.astype(BF16)

    def step(t, _):
        dt = t - 1
        chips = jnp.where((dt == 0) | (dt == half), 1, 2)

        def over(units, core_kind):
            def one(i, _):
                chip = lax.rem(jnp.where(i == 0, z - dt, z + dt) + nz, nz)
                if core_kind is not None:
                    way = jnp.where(dt == half, CORE_LAST[core_kind], i)
                    core_recv(core_kind, way, dt, chip).wait_recv()
                for unit in units:
                    attend(unit, chip)
                return 0

            lax.fori_loop(0, chips, one, 0)

        more = t <= half
        over((0, 1), C_KV_N)
        pl.when(more)(lambda: pump(KV_N, t))

        @pl.when(t == half + 1)
        def _():
            pump(DN_Y, 1)
            head_group(0, lam_n_ref)
            for delta in range(1, ntp):
                a_send(0, delta).start()

        over((2,), C_KV_W)
        pl.when(more)(lambda: pump(KV_W, t))
        pl.when(t == half + 1)(lambda: pump(DN_1, 1))
        over((3,), None)
        pl.when(more)(lambda: pump(UP, t))
        pl.when(t == half + 1)(lambda: pump(DN_2, 1))

        @pl.when(t == half - 1)
        def _():
            for kind in (DN_Y, DN_1, DN_2):
                for d in range(2):
                    z_send(kind, d, 0).start()

        @pl.when(dt >= 1)
        def _():
            complete(Y_UP, C_UP, UP, dt)

        @pl.when(t == half // 2)
        def _():
            for d in range(2):
                x_recv(d).wait_recv()
                x_relay(d).start()
            o_core(1, True).start()

        pl.when(t == half // 2 + 1)(lambda: o_core(ntp - 1, True).start())

        @pl.when(t == half - 2)
        def _():
            for d in range(2):
                x_relayed(d).wait_recv()
            o_core(2, True).start()

        return 0

    lax.fori_loop(1, half + 2, step, 0)

    head_group(1, lam_w_ref)
    for delta in range(1, ntp):
        a_send(1, delta).start()

    relays = [(kind, t) for t in range(2, half + 1) for kind in (DN_Y, DN_1, DN_2)]

    def relay(count):
        for _ in range(min(count, len(relays))):
            kind, t = relays.pop(0)
            pump(kind, t)
            if kind == DN_1:
                complete(Y_DN, C_DN, DN_Y, t - 1)

    relay(6)
    all_of(outs.at[pl.ds(0, ntp - 1), 0], os_.at[0], or_.at[0]).wait_recv()
    all_of(resid.at[pl.ds(0, ntp - 1)], rs.at[0], rr.at[0]).wait_recv()
    all_of(att.at[pl.ds(0, ntp - 1)], as_.at[0], ar.at[0]).wait_recv()

    width = mid.shape[1]
    squares = jnp.zeros((mid.shape[0], 128), F32)
    for n in range(0, width, COLS):
        cols = pl.ds(n, COLS)
        total = resid[:, :, cols].reshape(mid.shape[0], COLS).astype(F32)
        terms = jnp.zeros((mid.shape[0], COLS), F32)
        for peer in range(ntp):
            term = jnp.dot(att[peer, 0], outs[peer, 0, :, cols], preferred_element_type=F32)
            term = term + jnp.dot(att[peer, 1], outs[peer, 1, :, cols], preferred_element_type=F32)
            terms = terms + term.astype(BF16).astype(F32)
        total = (total + terms).astype(BF16)
        mid[:, cols] = total
        total = total.astype(F32)
        total = total * total
        for k in range(0, COLS, 128):
            squares = squares + total[:, k : k + 128]
        sumsq[...] = squares
        relay(1)
        squares = sumsq[...]

    inverse = lax.rsqrt(jnp.sum(squares, axis=1, keepdims=True) * (1.0 / width) + NORM_EPS)
    for k in range(width // 128):
        cols = pl.ds(128 * k, 128)
        gain = norm_gain_ref[k : k + 1, :].astype(F32)
        nrm[:, cols] = (mid[:, cols].astype(F32) * inverse * gain).astype(BF16)
    relay(1)

    all_of(up.at[pl.ds(0, nz)], cs.at[C_UP], cu.at[0]).wait_recv()
    for n in range(0, act.shape[1], COLS):
        cols = pl.ds(n, COLS)
        weights = up[:, :, cols].reshape(width, COLS)
        lifted = jnp.dot(nrm[...], weights, preferred_element_type=F32)
        lifted = jnp.maximum(lifted, 0.0)
        act[:, cols] = (lifted * lifted).astype(BF16)
        relay(1)

    def chips_of(t):
        if t in (0, half):
            return [(0 if t == 0 else 1, chip_at(1, t))]
        return [(d, chip_at(d, t)) for d in range(2)]

    def lower(t):
        weights = []
        for d, chip in chips_of(t):
            core_recv(C_DN, d, t, chip).wait_recv()
            weights.append(dn[pl.ds(2 * chip, 2)].reshape(2 * wrows, dn.shape[2]))
        weights = weights[0] if len(weights) == 1 else jnp.concatenate(weights, axis=0)
        lowered = lax.dot_general(
            act[...], weights, (((1,), (1,)), ((), ())), preferred_element_type=F32
        ).astype(BF16)
        for i in range(len(chips_of(t))):
            part[max(2 * t - 1, 0) + i] = lowered[:, 2 * wrows * i : 2 * wrows * (i + 1)]

    own = pl.ds(pl.multiple_of(own_rows * j, own_rows), own_rows)

    def finish(group):
        for delta in range(1, ntp):
            m_send(delta, group).wait_recv()
        for t in GROUPS[group]:
            for i, (_, chip) in enumerate(chips_of(t)):
                o = max(2 * t - 1, 0) + i
                cols = pl.ds(pl.multiple_of(chip * 2 * wrows, 2 * wrows), 2 * wrows)
                total = part[o, own].astype(F32)
                for delta in range(1, ntp):
                    total = total + mix[delta - 1, o].astype(F32)
                out_ref[:, cols] = (mid[own, cols].astype(F32) + total).astype(BF16)

    for group, distances in enumerate(GROUPS):
        for t in distances:
            lower(t)
            relay(1 if t < 4 else 2)
            if t == 5:
                complete(Y_DN, C_DN, DN_Y, half)
        for delta in range(1, ntp):
            m_send(delta, group).start()
        if group > 0:
            finish(group - 1)
    finish(len(GROUPS) - 1)

    blocks = nz - 1
    for kind in (KV_N, KV_W):
        parts = pl.ds(0, 2 if kind == KV_N else 3)
        all_of(kv.at[pl.ds(0, blocks), parts], zs.at[kind], cu.at[0]).wait_send()
        all_of(kv.at[pl.ds(0, nz), parts], cs.at[kind], cu.at[0]).wait_send()
    all_of(up.at[pl.ds(0, blocks), pl.ds(0, hrows)], zs.at[UP], cu.at[0]).wait_send()
    all_of(up.at[pl.ds(0, blocks), pl.ds(0, hrows)], ys.at[Y_UP], cu.at[0]).wait_send()
    for kind in (DN_Y, DN_1, DN_2):
        all_of(dn.at[pl.ds(0, blocks), pl.ds(0, qrows)], zs.at[kind], cu.at[0]).wait_send()
    all_of(dn.at[pl.ds(0, blocks), pl.ds(0, qrows)], ys.at[Y_DN], cu.at[0]).wait_send()
    all_of(up.at[pl.ds(0, nz)], cs.at[C_UP], cu.at[0]).wait_send()
    all_of(dn.at[pl.ds(0, nz)], cs.at[C_DN], cu.at[0]).wait_send()
    for d in range(2):
        x_send(d).wait_send()
        x_relay(d).wait_send()
    all_of(outs.at[pl.ds(0, ntp - 1), 0], os_.at[0], or_.at[0]).wait_send()
    all_of(resid.at[pl.ds(0, ntp - 1)], rs.at[0], rr.at[0]).wait_send()
    all_of(att.at[pl.ds(0, ntp - 1)], as_.at[0], ar.at[0]).wait_send()
    all_of(mix, ms.at[0], mr.at[0, 0]).wait_send()


def shards(
    nsp, ntp,
    resid_in, query_narrow, key_narrow, value_narrow, query_wide, key_wide, value_wide,
    lambda_narrow, lambda_wide, head_gain, out_narrow, out_wide, norm_gain, up_weight, down_weight,
):
    rows, heads, full = query_narrow.shape
    narrow, wide = full // 2, query_wide.shape[2] // 2
    width = resid_in.shape[1]
    hidden = up_weight.shape[1]
    nz = nsp // 2
    anywhere = pl.BlockSpec(memory_space=pl.ANY)
    vmem = pl.BlockSpec(memory_space=pltpu.VMEM)
    smem = pl.BlockSpec(memory_space=pltpu.SMEM)
    dma = pltpu.SemaphoreType.DMA
    own_rows = resid_in.shape[0]
    out_rows = out_narrow.shape[0]
    down = down_weight.T
    return pl.pallas_call(
        functools.partial(layer_kernel, nz, ntp, (narrow, narrow, wide, wide)),
        out_shape=jax.ShapeDtypeStruct(resid_in.shape, BF16),
        in_specs=[anywhere] * 11 + [smem, smem, vmem, vmem],
        out_specs=vmem,
        scratch_shapes=[
            pltpu.VMEM(query_narrow.shape, BF16),
            pltpu.VMEM(query_wide.shape, BF16),
            pltpu.VMEM((4, heads * rows, wide), BF16),
            pltpu.VMEM((nsp, 5, rows, wide), BF16),
            pltpu.VMEM((nsp, up_weight.shape[0], hidden), BF16),
            pltpu.VMEM((nsp, down.shape[0], hidden), BF16),
            pltpu.VMEM((ntp, 2, out_rows, width), BF16),
            pltpu.VMEM((ntp, own_rows, width), BF16),
            pltpu.VMEM((4, heads * rows, 2 * wide), F32),
            pltpu.VMEM((4, heads * rows, 128), F32),
            pltpu.VMEM((ntp, 2, rows, out_rows), BF16),
            pltpu.VMEM((rows, width), BF16),
            pltpu.VMEM((rows, width), BF16),
            pltpu.VMEM((rows, hidden), BF16),
            pltpu.VMEM((nz, rows, 2 * down.shape[0]), BF16),
            pltpu.VMEM((ntp - 1, nz, own_rows, 2 * down.shape[0]), BF16),
            pltpu.VMEM((rows, 128), F32),
            dma((6,)),
            dma((6, nz - 1)),
            dma((4,)),
            dma((3, nz)),
            dma((1,)),
            dma((2,)),
            dma((2, nz - 1)),
            dma((4,)),
            dma((4,)),
            dma((1,)),
            dma((1,)),
            dma((1,)),
            dma((1,)),
            dma((1,)),
            dma((1,)),
            dma((1,)),
            dma((ntp - 1, len(GROUPS))),
            dma((7,)),
        ],
        compiler_params=pltpu.CompilerParams(
            collective_id=0, has_side_effects=True, vmem_limit_bytes=62 * 1024 * 1024
        ),
        name="layer",
    )(
        query_narrow,
        query_wide,
        key_narrow.reshape(rows, full),
        value_narrow.reshape(rows, -1),
        key_wide.reshape(rows, 2 * wide),
        value_wide.reshape(rows, -1),
        up_weight,
        down,
        out_narrow,
        out_wide,
        resid_in,
        lambda_narrow,
        lambda_wide,
        head_gain.reshape(1, -1),
        norm_gain.reshape(-1, 128),
    )


def solution(mesh):
    placed = (
        P(("grp", "sp", "tp"), None),
        P(("grp", "sp"), "tp", None),
        P(("grp", "sp"), "tp", None),
        P(("grp", "sp"), "tp", None),
        P(("grp", "sp"), "tp", None),
        P(("grp", "sp"), "tp", None),
        P(("grp", "sp"), "tp", None),
        P("tp"),
        P("tp"),
        P(),
        P("tp", None),
        P("tp", None),
        P(),
        P("sp", "tp"),
        P("tp", "sp"),
    )
    return jax.shard_map(
        functools.partial(shards, mesh.shape["sp"], mesh.shape["tp"]),
        mesh=mesh,
        in_specs=placed,
        out_specs=P(("grp", "sp", "tp"), None),
        check_vma=False,
    )
```

```python
import functools
import math

import jax
import jax.numpy as jnp
from jax import lax
from jax.experimental import pallas as pl
from jax.experimental.pallas import tpu as pltpu
from jax.sharding import PartitionSpec as P

NORM_EPS = 1e-06
OUT_SCALE = 0.8
LOG2E = math.log2(math.e)
MESH = pl.DeviceIdType.MESH
BF16 = jnp.bfloat16
F32 = jnp.float32

KV_N, KV_W, UP, DN_Y, DN_1, DN_2 = range(6)
LAST_WAY = (1, 0, 1, 1, 0, 0)
C_KV_N, C_KV_W, C_DN, C_UP = range(4)
CORE_LAST = (1, 0, 1, 1)
Y_UP, Y_DN = range(2)
KEY_PART = (0, 0, 2, 3)
VALUE_PART = (1, 1, 4, 4)
Q_TILE = 128
COLS = 512
GROUPS = ((0, 1, 2), (3, 4), (5, 6), (7,), (8,))


def layer_kernel(
    nz, ntp, widths,
    qn_ref, qw_ref, kn_ref, vn_ref, kw_ref, vw_ref, up_ref, dn_ref, on_ref, ow_ref, res_ref,
    lam_n_ref, lam_w_ref, head_gain_ref, norm_gain_ref,
    out_ref,
    qn, qw, q, kv, up, dn, outs, resid, acc, top, att, mid, nrm, act, part, mix, sumsq,
    zs, zr, cs, cr, cu, ys, yr, xs, xr, os_, or_, rs, rr, as_, ar, ms, mr, ls,
):
    g, s, j = lax.axis_index("grp"), lax.axis_index("sp"), lax.axis_index("tp")
    z, c = s // 2, s % 2
    par = g % 2
    half = nz // 2
    rows = kv.shape[2]
    wrows = up.shape[1]
    hrows = wrows // 2
    qrows = wrows // 4
    own_rows = resid.shape[1]

    def sp_of(chip):
        return {"sp": 2 * lax.rem(chip + nz, nz) + c}

    z_to = (sp_of(z + 1), sp_of(z - 1))
    core_to = {"sp": 2 * z + 1 - c}
    y_to = {"grp": g + 1 - 2 * par}

    def tp_at(delta):
        return lax.rem(j + delta + ntp, ntp)

    def chip_at(d, t):
        return lax.rem(z - t + nz, nz) if d == 0 else lax.rem(z + t, nz)

    def slot(d, t):
        if isinstance(t, int) and isinstance(d, int):
            return 0 if t == 0 else 2 * half - 1 if t == half else 2 * t - 1 + d
        return jnp.where(t == 0, 0, jnp.where(t == half, 2 * half - 1, 2 * t - 1 + d))

    def piece(kind, block):
        if kind == KV_N:
            return kv.at[block, pl.ds(0, 2)]
        if kind == KV_W:
            return kv.at[block, pl.ds(2, 3)]
        if kind == UP:
            return up.at[block, pl.ds(pl.multiple_of(hrows * par, hrows), hrows)]
        if kind in (DN_1, DN_2):
            return dn.at[block, pl.ds(qrows * (1 + kind - DN_1), qrows)]
        return dn.at[block, pl.ds(pl.multiple_of(3 * qrows * par, qrows), qrows)]

    def remote(src, dst, send, recv, to):
        return pltpu.make_async_remote_copy(src, dst, send, recv, device_id=to, device_id_type=MESH)

    def z_send(kind, d, t):
        ref = piece(kind, 2 * chip_at(d, t) + c)
        return remote(ref, ref, zs.at[kind], zr.at[kind, slot(d, t + 1) - 1], z_to[d])

    def z_recv(kind, d, t):
        ref = piece(kind, 2 * chip_at(d, t) + c)
        return remote(ref, ref, zs.at[kind], zr.at[kind, slot(d, t) - 1], z_to[d])

    def core_piece(kind, block):
        if kind == C_KV_N:
            return kv.at[block, pl.ds(0, 2)]
        if kind == C_KV_W:
            return kv.at[block, pl.ds(2, 3)]
        return (up if kind == C_UP else dn).at[block]

    def core_got(kind, d, t):
        return cu.at[0] if kind == C_UP else cr.at[kind, slot(d, t)]

    def core_send(kind, d, t):
        ref = core_piece(kind, 2 * chip_at(d, t) + c)
        return remote(ref, ref, cs.at[kind], core_got(kind, d, t), core_to)

    def core_part(ref, d, t):
        return remote(ref, ref, cs.at[C_DN], core_got(C_DN, d, t), core_to)

    def core_recv(kind, d, t, chip):
        ref = core_piece(kind, 2 * chip + 1 - c)
        return remote(ref, ref, cs.at[kind], core_got(kind, d, t), core_to)

    def y_piece(kind, block, side):
        if kind == Y_UP:
            return up.at[block, pl.ds(pl.multiple_of(hrows * side, hrows), hrows)]
        return dn.at[block, pl.ds(pl.multiple_of(3 * qrows * side, qrows), qrows)]

    def y_send(kind, d, t):
        ref = y_piece(kind, 2 * chip_at(d, t) + c, par)
        return remote(ref, ref, ys.at[kind], yr.at[kind, slot(d, t) - 1], y_to)

    def y_recv(kind, d, t):
        ref = y_piece(kind, 2 * chip_at(d, t) + c, 1 - par)
        return remote(ref, ref, ys.at[kind], yr.at[kind, slot(d, t) - 1], y_to)

    def x_send(d):
        ref = outs.at[j, c]
        return remote(ref, ref, xs.at[d], xr.at[d], {"tp": tp_at(1 - 2 * d)})

    def x_recv(d):
        ref = outs.at[tp_at(2 * d - 1), c]
        return remote(ref, ref, xs.at[d], xr.at[d], {"tp": tp_at(1 - 2 * d)})

    def x_half(owner, d):
        n = outs.shape[2] // 2
        return outs.at[owner, c, pl.ds(n * d, n)]

    def x_relay(d):
        ref = x_half(tp_at(2 * d - 1), d)
        return remote(ref, ref, xs.at[2 + d], xr.at[2 + d], {"tp": tp_at(1 - 2 * d)})

    def x_relayed(d):
        ref = x_half(tp_at(2), d)
        return remote(ref, ref, xs.at[2 + d], xr.at[2 + d], {"tp": tp_at(1 - 2 * d)})

    def o_core(delta, mine):
        ref = outs.at[tp_at(delta), c if mine else 1 - c]
        return remote(ref, ref, os_.at[0], or_.at[0], core_to)

    def r_send(delta):
        ref = resid.at[j]
        return remote(ref, ref, rs.at[0], rr.at[0], {"tp": tp_at(delta)})

    def r_recv(delta):
        ref = resid.at[tp_at(-delta)]
        return remote(ref, ref, rs.at[0], rr.at[0], {"tp": tp_at(delta)})

    def a_send(kind, delta):
        ref = att.at[j, kind]
        return remote(ref, ref, as_.at[0], ar.at[0], {"tp": tp_at(delta)})

    def a_recv(kind, delta):
        ref = att.at[tp_at(-delta), kind]
        return remote(ref, ref, as_.at[0], ar.at[0], {"tp": tp_at(delta)})

    def m_send(delta, group):
        first = max(2 * GROUPS[group][0] - 1, 0)
        count = min(2 * GROUPS[group][-1], nz - 1) + 1 - first
        rows_to = pl.ds(pl.multiple_of(own_rows * tp_at(delta), own_rows), own_rows)
        src = part.at[pl.ds(first, count), rows_to]
        dst = mix.at[delta - 1, pl.ds(first, count)]
        return remote(src, dst, ms.at[0], mr.at[delta - 1, group], {"tp": tp_at(delta)})

    def all_of(ref, send, recv):
        return remote(ref, ref, send, recv, core_to)

    def takes(kind, d, t):
        return t <= (half if LAST_WAY[kind] == d else half - 1)

    def passes(kind, d, t):
        return t <= (half - 1 if LAST_WAY[kind] == d else half - 2)

    def when(condition, run):
        if isinstance(condition, bool):
            if condition:
                run()
        else:
            pl.when(condition)(run)

    barrier = pltpu.get_barrier_semaphore()
    friends = [z_to[0], z_to[1], core_to, y_to] + [{"tp": tp_at(k)} for k in range(1, ntp)]
    for friend in friends:
        pl.semaphore_signal(barrier, inc=1, device_id=friend, device_id_type=MESH)
    kd = kv.shape[3]
    local = [
        pltpu.make_async_copy(src, dst, ls.at[i])
        for src, dst, i in [
            (kn_ref, kv.at[s, 0], 0),
            (vn_ref, kv.at[s, 1], 0),
            (kw_ref.at[:, pl.ds(0, kd)], kv.at[s, 2], 0),
            (kw_ref.at[:, pl.ds(kd, kd)], kv.at[s, 3], 0),
            (vw_ref, kv.at[s, 4], 0),
            (up_ref, up.at[s], 1),
            (on_ref, outs.at[j, 0], 2),
            (ow_ref, outs.at[j, 1], 2),
            (res_ref, resid.at[j], 3),
            (dn_ref, dn.at[s], 4),
            (qn_ref, qn, 5),
            (qw_ref, qw, 6),
        ]
    ]
    for copy in local:
        copy.start()

    def local_wait(ref, i):
        pltpu.make_async_copy(ref, ref, ls.at[i]).wait()

    pl.semaphore_wait(barrier, len(friends))
    local_wait(kv.at[s], 0)
    for kind in (KV_N, KV_W):
        for d in range(2):
            z_send(kind, d, 0).start()
        core_send((C_KV_N, C_KV_W)[kind], 0, 0).start()
    local_wait(up.at[s], 1)
    for d in range(2):
        z_send(UP, d, 0).start()
    core_send(C_UP, 0, 0).start()
    local_wait(outs.at[j], 2)
    for d in range(2):
        x_send(d).start()
    local_wait(resid.at[j], 3)
    for delta in range(1, ntp):
        r_send(delta).start()
    local_wait(dn.at[s], 4)
    core_send(C_DN, 0, 0).start()

    acc[...] = jnp.zeros_like(acc)
    top[...] = jnp.full_like(top, -jnp.inf)
    local_wait(qn, 5)
    local_wait(qw, 6)
    narrow_q = qn[...].astype(F32)
    wide_q = qw[...].astype(F32)
    first_map = lax.broadcasted_iota(jnp.int32, (rows, kd), 1) < kd // 2
    for h in range(2):
        tile = pl.ds(h * rows, rows)
        head = narrow_q[:, h, :]
        q[0, tile] = jnp.where(first_map, head, 0.0).astype(BF16)
        q[1, tile] = jnp.where(first_map, 0.0, head).astype(BF16)
        head = wide_q[:, h, :].astype(BF16)
        q[2, tile] = head[:, :kd]
        q[3, tile] = head[:, kd:]

    def pump(kind, t):
        for d in range(2):

            def arrived(d=d):
                z_recv(kind, d, t).wait_recv()

                def forward():
                    z_send(kind, d, t).start()

                when(passes(kind, d, t), forward)
                if kind in (KV_N, KV_W):
                    core_send((C_KV_N, C_KV_W)[kind], d, t).start()
                if kind == UP:
                    y_send(Y_UP, d, t).start()
                if kind == DN_Y:
                    y_send(Y_DN, d, t).start()
                if kind in (DN_Y, DN_1, DN_2):
                    core_part(piece(kind, 2 * chip_at(d, t) + c), d, t).start()

            when(takes(kind, d, t), arrived)

    def complete(y_kind, core_kind, kind, t):
        for d in range(2):

            def done(d=d):
                y_recv(y_kind, d, t).wait_recv()
                if core_kind == C_DN:
                    core_part(y_piece(Y_DN, 2 * chip_at(d, t) + c, 1 - par), d, t).start()
                else:
                    core_send(core_kind, d, t).start()

            when(takes(kind, d, t), done)

    ones = jnp.ones((2 * rows, acc.shape[2] - kd), BF16)

    def attend(unit, chip):
        scale = widths[unit] ** -0.5 * LOG2E
        keys = kv[pl.ds(2 * chip, 2), KEY_PART[unit]].reshape(2 * rows, kd)
        values = kv[pl.ds(2 * chip, 2), VALUE_PART[unit]].reshape(2 * rows, kd)
        values = jnp.concatenate([values, ones], axis=1)
        lanes = top.shape[2]
        for row in range(0, q.shape[1], Q_TILE):
            tile = pl.ds(row, Q_TILE)
            scores = lax.dot_general(
                q[unit, tile], keys, (((1,), (1,)), ((), ())), preferred_element_type=F32
            )
            old = top[unit, tile]
            new = jnp.maximum(old, jnp.max(scores, axis=1, keepdims=True))
            rescale = jnp.exp2((old - new) * scale)
            top[unit, tile] = new
            wide = jnp.concatenate([new] * (2 * rows // lanes), axis=1)
            powers = jnp.exp2((scores - wide) * scale).astype(BF16)
            weighted = jnp.dot(powers, values, preferred_element_type=F32)
            wide = jnp.concatenate([rescale] * (acc.shape[2] // lanes), axis=1)
            acc[unit, tile] = acc[unit, tile] * wide + weighted

    def head_group(kind, lam_ref):
        for h in range(2):
            tile = pl.ds(h * rows, rows)
            one = acc[2 * kind, tile]
            two = acc[2 * kind + 1, tile]
            diff = one[:, :kd] / one[:, kd:] - lam_ref[h] * (two[:, :kd] / two[:, kd:])
            square = jnp.mean(diff * diff, axis=-1, keepdims=True)
            diff = diff * lax.rsqrt(square + NORM_EPS) * head_gain_ref[...] * OUT_SCALE
            att[j, kind, :, pl.ds(h * kd, kd)] = diff.astype(BF16)

    def step(t, _):
        dt = t - 1
        chips = jnp.where((dt == 0) | (dt == half), 1, 2)

        def over(units, core_kind):
            def one(i, _):
                chip = lax.rem(jnp.where(i == 0, z - dt, z + dt) + nz, nz)
                if core_kind is not None:
                    way = jnp.where(dt == half, CORE_LAST[core_kind], i)
                    core_recv(core_kind, way, dt, chip).wait_recv()
                for unit in units:
                    attend(unit, chip)
                return 0

            lax.fori_loop(0, chips, one, 0)

        more = t <= half
        over((0, 1), C_KV_N)
        pl.when(more)(lambda: pump(KV_N, t))

        @pl.when(t == half + 1)
        def _():
            pump(DN_Y, 1)
            head_group(0, lam_n_ref)
            for delta in range(1, ntp):
                a_send(0, delta).start()

        over((2,), C_KV_W)
        pl.when(more)(lambda: pump(KV_W, t))
        pl.when(t == half + 1)(lambda: pump(DN_1, 1))
        over((3,), None)
        pl.when(more)(lambda: pump(UP, t))
        pl.when(t == half + 1)(lambda: pump(DN_2, 1))

        @pl.when(t == half - 1)
        def _():
            for kind in (DN_Y, DN_1, DN_2):
                for d in range(2):
                    z_send(kind, d, 0).start()

        @pl.when(dt >= 1)
        def _():
            complete(Y_UP, C_UP, UP, dt)

        @pl.when(t == half // 2)
        def _():
            for d in range(2):
                x_recv(d).wait_recv()
                x_relay(d).start()
            o_core(1, True).start()

        pl.when(t == half // 2 + 1)(lambda: o_core(ntp - 1, True).start())

        @pl.when(t == half - 2)
        def _():
            for d in range(2):
                x_relayed(d).wait_recv()
            o_core(2, True).start()

        return 0

    lax.fori_loop(1, half + 2, step, 0)

    head_group(1, lam_w_ref)
    for delta in range(1, ntp):
        a_send(1, delta).start()

    relays = [(kind, t) for t in range(2, half + 1) for kind in (DN_Y, DN_1, DN_2)]

    def relay(count):
        for _ in range(min(count, len(relays))):
            kind, t = relays.pop(0)
            pump(kind, t)
            if kind == DN_1:
                complete(Y_DN, C_DN, DN_Y, t - 1)

    relay(6)
    all_of(outs.at[pl.ds(0, ntp - 1), 0], os_.at[0], or_.at[0]).wait_recv()
    all_of(resid.at[pl.ds(0, ntp - 1)], rs.at[0], rr.at[0]).wait_recv()
    all_of(att.at[pl.ds(0, ntp - 1)], as_.at[0], ar.at[0]).wait_recv()

    width = mid.shape[1]
    squares = jnp.zeros((mid.shape[0], 128), F32)
    for n in range(0, width, COLS):
        cols = pl.ds(n, COLS)
        total = resid[:, :, cols].reshape(mid.shape[0], COLS).astype(F32)
        terms = jnp.zeros((mid.shape[0], COLS), F32)
        for peer in range(ntp):
            term = jnp.dot(att[peer, 0], outs[peer, 0, :, cols], preferred_element_type=F32)
            term = term + jnp.dot(att[peer, 1], outs[peer, 1, :, cols], preferred_element_type=F32)
            terms = terms + term.astype(BF16).astype(F32)
        total = (total + terms).astype(BF16)
        mid[:, cols] = total
        total = total.astype(F32)
        total = total * total
        for k in range(0, COLS, 128):
            squares = squares + total[:, k : k + 128]
        sumsq[...] = squares
        relay(1)
        squares = sumsq[...]

    inverse = lax.rsqrt(jnp.sum(squares, axis=1, keepdims=True) * (1.0 / width) + NORM_EPS)
    for k in range(width // 128):
        cols = pl.ds(128 * k, 128)
        gain = norm_gain_ref[k : k + 1, :].astype(F32)
        nrm[:, cols] = (mid[:, cols].astype(F32) * inverse * gain).astype(BF16)
    relay(1)

    all_of(up.at[pl.ds(0, nz)], cs.at[C_UP], cu.at[0]).wait_recv()
    for n in range(0, act.shape[1], COLS):
        cols = pl.ds(n, COLS)
        weights = up[:, :, cols].reshape(width, COLS)
        lifted = jnp.dot(nrm[...], weights, preferred_element_type=F32)
        lifted = jnp.maximum(lifted, 0.0)
        act[:, cols] = (lifted * lifted).astype(BF16)
        relay(1)

    def chips_of(t):
        if t in (0, half):
            return [(0 if t == 0 else 1, chip_at(1, t))]
        return [(d, chip_at(d, t)) for d in range(2)]

    def lower(t):
        weights = []
        for d, chip in chips_of(t):
            core_recv(C_DN, d, t, chip).wait_recv()
            weights.append(dn[pl.ds(2 * chip, 2)].reshape(2 * wrows, dn.shape[2]))
        weights = weights[0] if len(weights) == 1 else jnp.concatenate(weights, axis=0)
        lowered = lax.dot_general(
            act[...], weights, (((1,), (1,)), ((), ())), preferred_element_type=F32
        ).astype(BF16)
        for i in range(len(chips_of(t))):
            part[max(2 * t - 1, 0) + i] = lowered[:, 2 * wrows * i : 2 * wrows * (i + 1)]

    own = pl.ds(pl.multiple_of(own_rows * j, own_rows), own_rows)

    def finish(group):
        for delta in range(1, ntp):
            m_send(delta, group).wait_recv()
        for t in GROUPS[group]:
            for i, (_, chip) in enumerate(chips_of(t)):
                o = max(2 * t - 1, 0) + i
                cols = pl.ds(pl.multiple_of(chip * 2 * wrows, 2 * wrows), 2 * wrows)
                total = part[o, own].astype(F32)
                for delta in range(1, ntp):
                    total = total + mix[delta - 1, o].astype(F32)
                out_ref[:, cols] = (mid[own, cols].astype(F32) + total).astype(BF16)

    for group, distances in enumerate(GROUPS):
        for t in distances:
            lower(t)
            relay(1 if t < 4 else 2)
            if t == 5:
                complete(Y_DN, C_DN, DN_Y, half)
        for delta in range(1, ntp):
            m_send(delta, group).start()
        if group > 0:
            finish(group - 1)
    finish(len(GROUPS) - 1)

    blocks = nz - 1
    for kind in (KV_N, KV_W):
        parts = pl.ds(0, 2 if kind == KV_N else 3)
        all_of(kv.at[pl.ds(0, blocks), parts], zs.at[kind], cu.at[0]).wait_send()
        all_of(kv.at[pl.ds(0, nz), parts], cs.at[kind], cu.at[0]).wait_send()
    all_of(up.at[pl.ds(0, blocks), pl.ds(0, hrows)], zs.at[UP], cu.at[0]).wait_send()
    all_of(up.at[pl.ds(0, blocks), pl.ds(0, hrows)], ys.at[Y_UP], cu.at[0]).wait_send()
    for kind in (DN_Y, DN_1, DN_2):
        all_of(dn.at[pl.ds(0, blocks), pl.ds(0, qrows)], zs.at[kind], cu.at[0]).wait_send()
    all_of(dn.at[pl.ds(0, blocks), pl.ds(0, qrows)], ys.at[Y_DN], cu.at[0]).wait_send()
    all_of(up.at[pl.ds(0, nz)], cs.at[C_UP], cu.at[0]).wait_send()
    all_of(dn.at[pl.ds(0, nz)], cs.at[C_DN], cu.at[0]).wait_send()
    for d in range(2):
        x_send(d).wait_send()
        x_relay(d).wait_send()
    all_of(outs.at[pl.ds(0, ntp - 1), 0], os_.at[0], or_.at[0]).wait_send()
    all_of(resid.at[pl.ds(0, ntp - 1)], rs.at[0], rr.at[0]).wait_send()
    all_of(att.at[pl.ds(0, ntp - 1)], as_.at[0], ar.at[0]).wait_send()
    all_of(mix, ms.at[0], mr.at[0, 0]).wait_send()


def shards(
    nsp, ntp,
    resid_in, query_narrow, key_narrow, value_narrow, query_wide, key_wide, value_wide,
    lambda_narrow, lambda_wide, head_gain, out_narrow, out_wide, norm_gain, up_weight, down_weight,
):
    rows, heads, full = query_narrow.shape
    narrow, wide = full // 2, query_wide.shape[2] // 2
    width = resid_in.shape[1]
    hidden = up_weight.shape[1]
    nz = nsp // 2
    anywhere = pl.BlockSpec(memory_space=pl.ANY)
    vmem = pl.BlockSpec(memory_space=pltpu.VMEM)
    smem = pl.BlockSpec(memory_space=pltpu.SMEM)
    dma = pltpu.SemaphoreType.DMA
    own_rows = resid_in.shape[0]
    out_rows = out_narrow.shape[0]
    down = down_weight.T
    return pl.pallas_call(
        functools.partial(layer_kernel, nz, ntp, (narrow, narrow, wide, wide)),
        out_shape=jax.ShapeDtypeStruct(resid_in.shape, BF16),
        in_specs=[anywhere] * 11 + [smem, smem, vmem, vmem],
        out_specs=vmem,
        scratch_shapes=[
            pltpu.VMEM(query_narrow.shape, BF16),
            pltpu.VMEM(query_wide.shape, BF16),
            pltpu.VMEM((4, heads * rows, wide), BF16),
            pltpu.VMEM((nsp, 5, rows, wide), BF16),
            pltpu.VMEM((nsp, up_weight.shape[0], hidden), BF16),
            pltpu.VMEM((nsp, down.shape[0], hidden), BF16),
            pltpu.VMEM((ntp, 2, out_rows, width), BF16),
            pltpu.VMEM((ntp, own_rows, width), BF16),
            pltpu.VMEM((4, heads * rows, 2 * wide), F32),
            pltpu.VMEM((4, heads * rows, 128), F32),
            pltpu.VMEM((ntp, 2, rows, out_rows), BF16),
            pltpu.VMEM((rows, width), BF16),
            pltpu.VMEM((rows, width), BF16),
            pltpu.VMEM((rows, hidden), BF16),
            pltpu.VMEM((nz, rows, 2 * down.shape[0]), BF16),
            pltpu.VMEM((ntp - 1, nz, own_rows, 2 * down.shape[0]), BF16),
            pltpu.VMEM((rows, 128), F32),
            dma((6,)),
            dma((6, nz - 1)),
            dma((4,)),
            dma((3, nz)),
            dma((1,)),
            dma((2,)),
            dma((2, nz - 1)),
            dma((4,)),
            dma((4,)),
            dma((1,)),
            dma((1,)),
            dma((1,)),
            dma((1,)),
            dma((1,)),
            dma((1,)),
            dma((1,)),
            dma((ntp - 1, len(GROUPS))),
            dma((7,)),
        ],
        compiler_params=pltpu.CompilerParams(
            collective_id=0, has_side_effects=True, vmem_limit_bytes=62 * 1024 * 1024
        ),
        name="layer",
    )(
        query_narrow,
        query_wide,
        key_narrow.reshape(rows, full),
        value_narrow.reshape(rows, -1),
        key_wide.reshape(rows, 2 * wide),
        value_wide.reshape(rows, -1),
        up_weight,
        down,
        out_narrow,
        out_wide,
        resid_in,
        lambda_narrow,
        lambda_wide,
        head_gain.reshape(1, -1),
        norm_gain.reshape(-1, 128),
    )


def solution(mesh):
    placed = (
        P(("grp", "sp", "tp"), None),
        P(("grp", "sp"), "tp", None),
        P(("grp", "sp"), "tp", None),
        P(("grp", "sp"), "tp", None),
        P(("grp", "sp"), "tp", None),
        P(("grp", "sp"), "tp", None),
        P(("grp", "sp"), "tp", None),
        P("tp"),
        P("tp"),
        P(),
        P("tp", None),
        P("tp", None),
        P(),
        P("sp", "tp"),
        P("tp", "sp"),
    )
    return jax.shard_map(
        functools.partial(shards, mesh.shape["sp"], mesh.shape["tp"]),
        mesh=mesh,
        in_specs=placed,
        out_specs=P(("grp", "sp", "tp"), None),
        check_vma=False,
    )
```
